32 devices in a mesh: sp: 16 (over z, y, core), tp: 2 (over x).
Axes of the slice: x: 2, y: 2, z: 4, core: 2. Of those that a mesh axis runs over, the one named last changes fastest.
Arguments:
- activations: bfloat16 [4096, 2048], P('sp', 'tp'), may hold values from -8 to 8
- norm_gain: float32 [2048], replicated, may hold values from 0.1 to 1.9
- win_query: bfloat16 [2048, 1024], P(None, 'tp'), may hold values from -1 to 1
- win_key: bfloat16 [2048, 512], P(None, 'tp'), may hold values from -1 to 1
- win_value: bfloat16 [2048, 512], P(None, 'tp'), may hold values from -0.125 to 0.125
- sink_logit: float32 [16], P('tp'), may hold values from 1 to 6
- lat_query: bfloat16 [2048, 1536], P(None, 'tp'), may hold values from -1 to 1
- key_value_down_weight: bfloat16 [2048, 128], replicated, may hold values from -0.125 to 0.125
- rope_key: bfloat16 [2048, 64], replicated, may hold values from -1 to 1
- latent_norm_gain: float32 [128], replicated, may hold values from 0.1 to 1.9
- key_up_weight: bfloat16 [128, 1024], P(None, 'tp'), may hold values from -0.5 to 0.5
- value_up_weight: bfloat16 [128, 1024], P(None, 'tp'), may hold values from -0.5 to 0.5
- out_win: bfloat16 [1024, 2048], P('tp'), may hold values from -0.359375 to 0.359375
- out_lat: bfloat16 [1024, 2048], P('tp'), may hold values from -0.59765625 to 0.59765625
Outputs:
- mixed: bfloat16 [4096, 2048], P('sp', 'tp')
The draws below stay inside these ranges and needn't reach their ends.
All inputs are finite; a program needn't handle non-finite values.
Results may differ from the reference program's by a relative error of at most 0.025.
Values may be sent and summed in bfloat16 or wider, within the bound.
No kernel may reach another device: no remote copies, remote signals or barrier semaphores. Data moves between devices by JAX's collectives and lax.ppermute only.
A program may use at most 64 MiB of HBM per device.

```python
import jax
import jax.numpy as jnp
from jax import lax

MODEL_WIDTH = 2048
HEADS_A = 16
KV_A = 8
DH = 64
WINDOW = 128
LATENT_HEADS = 8
LATENT_WIDTH = 128
UNROTATED_WIDTH = 128
D_ROPE = 64
VALUE_WIDTH = 128
TOK_DEV = 256
SEQ = 4096


def drawn(key, row_count, col_count, spread):
    values = jnp.clip(jax.random.normal(key, (row_count, col_count), jnp.float32) * spread, -1.0, 1.0)
    return values.astype(jnp.bfloat16)


def draw_activations(key, part):
    key_base = jax.random.fold_in(key, 11)
    values = jnp.clip(jax.random.normal(key_base, (SEQ, MODEL_WIDTH), jnp.float32), -6.0, 6.0)
    return values.astype(jnp.bfloat16)


def draw_win_query(key, part):
    return drawn(jax.random.fold_in(key, 21), MODEL_WIDTH, HEADS_A * DH, MODEL_WIDTH ** (-0.5))


def draw_win_key(key, part):
    return drawn(jax.random.fold_in(key, 22), MODEL_WIDTH, KV_A * DH, MODEL_WIDTH ** (-0.5))


def draw_lat_query(key, part):
    return drawn(jax.random.fold_in(key, 23), MODEL_WIDTH, LATENT_HEADS * (UNROTATED_WIDTH + D_ROPE), 2.5 * MODEL_WIDTH ** (-0.5))


def draw_rope_key(key, part):
    return drawn(jax.random.fold_in(key, 24), MODEL_WIDTH, D_ROPE, MODEL_WIDTH ** (-0.5))


def levels(stream_key, shape, split, least, largest):
    gain, own = 1.0, jax.random.fold_in(stream_key, 6)
    for position, shards_of in split:
        heights = jnp.exp(jax.random.uniform(jax.random.fold_in(own, position), (shards_of,), jnp.float32, least / len(split), largest / len(split)))
        gain = gain * jnp.repeat(heights, shape[position] // shards_of).reshape([-1 if axis == position else 1 for axis in range(len(shape))])
    return gain


def bell_draw(own_key, dims, scale, bound, shards=(), kind=jnp.bfloat16):
    result = jax.random.normal(own_key, dims, jnp.float32) * scale
    if len(shards) > 0:
        result = levels(own_key, dims, shards, -0.22, 0.18) * result
    return jnp.clip(result, min=-bound, max=bound).astype(kind)


def setup_inputs(seed: int = 0) -> dict:
    key_of = jax.random.split(jax.random.key(seed), 15)
    return {
        "activations": draw_activations(jax.random.fold_in(key_of[14], 71), 0),
        "norm_gain": jnp.clip(1.0 + 0.18 * jax.random.normal(key_of[1], (MODEL_WIDTH,), jnp.float32), 0.1, 1.9),
        "win_query": draw_win_query(jax.random.fold_in(key_of[14], 71), 0),
        "win_key": draw_win_key(jax.random.fold_in(key_of[14], 71), 0),
        "win_value": bell_draw(key_of[4], (MODEL_WIDTH, KV_A * DH), MODEL_WIDTH ** -0.5, 0.125, ((1, 2),)),
        "sink_logit": jnp.clip(1.0 + 5.0 * jax.random.uniform(key_of[5], (HEADS_A,), jnp.float32) ** levels(key_of[5], (HEADS_A,), ((0, 2),), -0.2, 0.2), 1.0, 6.0),
        "lat_query": draw_lat_query(jax.random.fold_in(key_of[14], 71), 0),
        "key_value_down_weight": bell_draw(key_of[7], (MODEL_WIDTH, LATENT_WIDTH), MODEL_WIDTH ** -0.5, 0.125),
        "rope_key": draw_rope_key(jax.random.fold_in(key_of[14], 71), 0),
        "latent_norm_gain": jnp.clip(1.0 + 0.18 * jax.random.normal(key_of[9], (LATENT_WIDTH,), jnp.float32), 0.1, 1.9),
        "key_up_weight": bell_draw(key_of[10], (LATENT_WIDTH, LATENT_HEADS * UNROTATED_WIDTH), LATENT_WIDTH ** -0.5, 0.5, ((1, 2),)),
        "value_up_weight": bell_draw(key_of[11], (LATENT_WIDTH, LATENT_HEADS * VALUE_WIDTH), LATENT_WIDTH ** -0.5, 0.5, ((1, 2),)),
        "out_win": bell_draw(key_of[12], (HEADS_A * DH, MODEL_WIDTH), 0.06, 0.359375, ((0, 2),)),
        "out_lat": bell_draw(key_of[13], (LATENT_HEADS * VALUE_WIDTH, MODEL_WIDTH), 0.1, 0.59765625, ((0, 2),)),
    }


EPSILON = 1e-06
ROPE_BASE = 10000.0

def rotate(vectors, angles):
    half_width = vectors.shape[-1] // 2
    cosine_table = jnp.cos(angles)
    sine_table = jnp.sin(angles)
    lower_half = vectors[..., :half_width]
    upper_half = vectors[..., half_width:]
    return jnp.concatenate([lower_half * cosine_table - upper_half * sine_table, lower_half * sine_table + upper_half * cosine_table], axis=-1)

def rotary_angles(places, width):
    frequency = 1.0 / ROPE_BASE ** (jnp.arange(0, width, 2).astype(jnp.float32) / width)
    return places[:, None] * frequency[None, :]

def reference(activations, norm_gain, win_query, win_key, win_value, sink_logit, lat_query, key_value_down_weight, rope_key, latent_norm_gain, key_up_weight, value_up_weight, out_win, out_lat):
    widened = activations.astype(jnp.float32)
    row_scale = lax.rsqrt(lax.optimization_barrier(jnp.mean(widened * widened, axis=1)) + EPSILON)[:, None]
    normalized = (widened * norm_gain[None, :]).astype(jnp.bfloat16)

    def project(weight):
        return jnp.dot(normalized, weight, preferred_element_type=jnp.float32)
    win_queries = (project(win_query) * row_scale).astype(jnp.bfloat16)
    win_keys = (project(win_key) * row_scale).astype(jnp.bfloat16)
    win_values = (project(win_value) * row_scale).astype(jnp.bfloat16)
    places = jnp.arange(SEQ).astype(jnp.float32)
    angles = rotary_angles(places, D_ROPE)
    query_all = (project(lat_query) * row_scale).reshape(SEQ, LATENT_HEADS, UNROTATED_WIDTH + D_ROPE)
    query_plain = query_all[..., :UNROTATED_WIDTH].astype(jnp.bfloat16)
    query_turned = rotate(query_all[..., UNROTATED_WIDTH:], angles[:, None, :]).astype(jnp.bfloat16)
    compressed = project(key_value_down_weight)
    latent = (compressed * lax.rsqrt(lax.optimization_barrier(jnp.mean(compressed * compressed, axis=1, keepdims=True)) + EPSILON) * latent_norm_gain[None, :]).astype(jnp.bfloat16)
    key_rotary = rotate(project(rope_key) * row_scale, angles).astype(jnp.bfloat16)
    key_nope = jnp.dot(latent, key_up_weight, preferred_element_type=jnp.float32).astype(jnp.bfloat16)
    value_lat = jnp.dot(latent, value_up_weight, preferred_element_type=jnp.float32).astype(jnp.bfloat16)
    block_count = SEQ // WINDOW
    groups = HEADS_A // KV_A
    query_blocks = win_queries.reshape(block_count, WINDOW, KV_A, groups, DH)
    zero_rim = jnp.zeros((WINDOW, KV_A * DH), jnp.bfloat16)
    key_padded = jnp.concatenate([zero_rim, win_keys, zero_rim], 0).reshape(block_count + 2, WINDOW, KV_A, DH)
    value_padded = jnp.concatenate([zero_rim, win_values, zero_rim], 0).reshape(block_count + 2, WINDOW, KV_A, DH)
    key_near = jnp.concatenate([key_padded[:-2], key_padded[1:-1], key_padded[2:]], axis=1)
    value_near = jnp.concatenate([value_padded[:-2], value_padded[1:-1], value_padded[2:]], axis=1)
    slopes = jnp.exp2(-8.0 * jnp.arange(1, HEADS_A + 1).astype(jnp.float32) / HEADS_A).reshape(KV_A, groups)
    sink_table = sink_logit.reshape(KV_A, groups)

    def window_block(inputs):
        query_block, key_block, value_block, block_index = inputs
        query_pos = block_index * WINDOW + jnp.arange(WINDOW, dtype=jnp.int32)
        key_pos = (block_index - 1) * WINDOW + jnp.arange(3 * WINDOW, dtype=jnp.int32)
        distance = jnp.abs(query_pos[:, None] - key_pos[None, :])
        in_window = (distance <= WINDOW) & (key_pos[None, :] >= 0) & (key_pos[None, :] < SEQ)
        scores = jnp.einsum('qhgd,khd->hgqk', query_block.astype(jnp.float32), key_block.astype(jnp.float32)) * DH ** (-0.5)
        scores = scores - slopes[:, :, None, None] * distance.astype(jnp.float32)[None, None]
        scores = jnp.where(in_window[None, None], scores, -jnp.inf)
        row_peak = jnp.maximum(lax.optimization_barrier(jnp.max(scores, axis=3)), sink_table[:, :, None])
        weights = jnp.exp(scores - row_peak[..., None])
        denominator = lax.optimization_barrier(jnp.sum(weights, axis=3)) + jnp.exp(sink_table[:, :, None] - row_peak)
        rounded = lax.optimization_barrier(weights.astype(jnp.bfloat16)).astype(jnp.float32)
        blended = jnp.einsum('hgqk,khd->qhgd', rounded, value_block.astype(jnp.float32))
        blended = blended / jnp.transpose(denominator, (2, 0, 1))[..., None]
        return blended.reshape(WINDOW, HEADS_A * DH).astype(jnp.bfloat16)
    win_out = lax.map(window_block, (query_blocks, key_near, value_near, jnp.arange(block_count, dtype=jnp.int32))).reshape(SEQ, HEADS_A * DH)
    span_count = SEQ // TOK_DEV
    plain_keys = key_nope.astype(jnp.float32).reshape(SEQ, LATENT_HEADS, UNROTATED_WIDTH)
    lat_values = value_lat.astype(jnp.float32).reshape(SEQ, LATENT_HEADS, VALUE_WIDTH)
    turned_keys = key_rotary.astype(jnp.float32)

    def latent_block(inputs):
        plain_block, turned_block = inputs
        scores = (jnp.einsum('qhd,khd->hqk', plain_block.astype(jnp.float32), plain_keys) + jnp.einsum('qhd,kd->hqk', turned_block.astype(jnp.float32), turned_keys)) * (UNROTATED_WIDTH + D_ROPE) ** (-0.5)
        row_peak = lax.optimization_barrier(jnp.max(scores, axis=2, keepdims=True))
        weights = jnp.exp(scores - row_peak)
        totals = lax.optimization_barrier(jnp.sum(weights, axis=2))
        rounded = lax.optimization_barrier(weights.astype(jnp.bfloat16)).astype(jnp.float32)
        blended = jnp.einsum('hqk,khd->qhd', rounded, lat_values) / jnp.transpose(totals)[..., None]
        return blended.reshape(TOK_DEV, LATENT_HEADS * VALUE_WIDTH).astype(jnp.bfloat16)
    lat_out = lax.map(latent_block, (query_plain.reshape(span_count, TOK_DEV, LATENT_HEADS, UNROTATED_WIDTH), query_turned.reshape(span_count, TOK_DEV, LATENT_HEADS, D_ROPE))).reshape(SEQ, LATENT_HEADS * VALUE_WIDTH)
    summed = jnp.dot(win_out, out_win, preferred_element_type=jnp.float32) + jnp.dot(lat_out, out_lat, preferred_element_type=jnp.float32)
    return summed.astype(jnp.bfloat16)
```

```python
from functools import partial

import jax
import jax.numpy as jnp
from jax import lax
from jax.experimental import pallas as pl
from jax.experimental.pallas import tpu as pltpu
from jax.sharding import PartitionSpec as P

HEADS_A = 16
DH = 64
WINDOW = 128
UNROTATED_WIDTH = 128
D_ROPE = 64
VALUE_WIDTH = 128


EPSILON = 1e-06
ROPE_BASE = 10000.0
LOG2E = 1.4426950408889634
LANES = 128
MASKED = -1e30


F32 = jnp.float32
BF16 = jnp.bfloat16


def padded_2(cells, sides, width):
    for axis, dim in sides:
        count = lax.axis_size(axis)
        ends = count - 1
        head = lax.slice_in_dim(cells, 0, width, axis=dim)
        tail = lax.slice_in_dim(cells, cells.shape[dim] - width, cells.shape[dim], axis=dim)
        cells = jnp.concatenate(
            [
                lax.ppermute(tail, axis, [(i, (i + 1) % count) for i in range(ends)]),
                cells,
                lax.ppermute(head, axis, [((i + 1) % count, i) for i in range(ends)]),
            ],
            axis=dim,
        )
    return cells


def rotate(vectors, angles):
    half_width = vectors.shape[-1] // 2
    cosine_table = jnp.cos(angles)
    sine_table = jnp.sin(angles)
    lower_half = vectors[..., :half_width]
    upper_half = vectors[..., half_width:]
    return jnp.concatenate(
        [
            lower_half * cosine_table - upper_half * sine_table,
            lower_half * sine_table + upper_half * cosine_table,
        ],
        axis=-1,
    )


def rotary_angles(places, width):
    frequency = 1.0 / ROPE_BASE ** (jnp.arange(0, width, 2).astype(jnp.float32) / width)
    return places[:, None] * frequency[None, :]


def window_attention(queries, padded, sinks, offset, seq_total, head_start):
    tok_rows = queries.shape[0]
    key_heads = padded.shape[1] // (2 * DH)
    groups = queries.shape[1] // (DH * key_heads)
    key_rows = padded[:, : key_heads * DH].reshape(-1, key_heads, DH)
    value_rows = padded[:, key_heads * DH :].reshape(-1, key_heads, DH)
    grouped = queries.reshape(tok_rows, key_heads, groups, DH)
    scores = jnp.einsum(
        "qhgd,khd->hgqk", grouped, key_rows, preferred_element_type=jnp.float32
    ) * DH ** (-0.5)
    query_pos = offset + jnp.arange(tok_rows, dtype=jnp.int32)
    key_pos = offset - WINDOW + jnp.arange(tok_rows + 2 * WINDOW, dtype=jnp.int32)
    distance = jnp.abs(query_pos[:, None] - key_pos[None, :])
    in_window = (distance <= WINDOW) & (key_pos[None, :] >= 0) & (key_pos[None, :] < seq_total)
    head_ids = head_start + jnp.arange(key_heads * groups, dtype=jnp.int32)
    slopes = jnp.exp2(-8.0 * (head_ids + 1).astype(jnp.float32) / HEADS_A).reshape(
        key_heads, groups
    )
    scores = scores - slopes[:, :, None, None] * distance.astype(jnp.float32)[None, None]
    scores = jnp.where(in_window[None, None], scores, -jnp.inf)
    sink_table = sinks.reshape(key_heads, groups)
    row_peak = jnp.maximum(jnp.max(scores, axis=3), sink_table[:, :, None])
    weights = jnp.exp(scores - row_peak[..., None])
    denominator = jnp.sum(weights, axis=3) + jnp.exp(sink_table[:, :, None] - row_peak)
    blended = jnp.einsum(
        "hgqk,khd->qhgd",
        weights.astype(jnp.bfloat16),
        value_rows,
        preferred_element_type=jnp.float32,
    )
    blended = blended / jnp.transpose(denominator, (2, 0, 1))[..., None]
    return blended.reshape(tok_rows, key_heads * groups * DH).astype(jnp.bfloat16)


def latent_step(running, key_block, query_plain, query_turned):
    row_peak, totals, weighted = running
    keys_plain, values_plain, keys_turned = key_block
    key_count = keys_plain.shape[0]
    head_count = query_plain.shape[1]
    scores = jnp.einsum(
        "qhd,khd->hqk",
        query_plain,
        keys_plain.reshape(key_count, head_count, UNROTATED_WIDTH),
        preferred_element_type=jnp.float32,
    )
    scores = scores + jnp.einsum(
        "qhd,kd->hqk", query_turned, keys_turned, preferred_element_type=jnp.float32
    )
    scores = scores * (UNROTATED_WIDTH + D_ROPE) ** (-0.5)
    new_peak = jnp.maximum(row_peak, jnp.max(scores, axis=2))
    factor = jnp.exp(row_peak - new_peak)
    weights = jnp.exp(scores - new_peak[..., None])
    totals = totals * factor + jnp.sum(weights, axis=2)
    weighted = weighted * factor[..., None] + jnp.einsum(
        "hqk,khd->hqd",
        weights.astype(jnp.bfloat16),
        values_plain.reshape(key_count, head_count, VALUE_WIDTH),
        preferred_element_type=jnp.float32,
    )
    return (new_peak, totals, weighted)


def over_blocks(running, pieces, prepare, attend, block_rows):
    key_count = pieces[0].shape[0]
    stacked = tuple(
        (
            piece_part.reshape((key_count // block_rows, block_rows) + piece_part.shape[1:])
            for piece_part in pieces
        )
    )

    def one_block(state_now, key_block):
        return (attend(state_now, prepare(key_block)), None)

    return lax.scan(one_block, running, stacked)[0]


def per_device_wide(
    activations,
    norm_gain,
    win_query,
    win_key,
    win_value,
    sink_logit,
    lat_query,
    key_value_down_weight,
    rope_key,
    latent_norm_gain,
    key_up_weight,
    value_up_weight,
    out_win,
    out_lat,
):
    tok_rows = activations.shape[0]
    weights_all = (win_query, win_key, win_value, lat_query, key_value_down_weight, rope_key)
    widened = lax.all_gather(activations, "tp", axis=1, tiled=True).astype(jnp.float32)
    normalized = (widened * norm_gain[None, :]).astype(jnp.bfloat16)
    squares = jnp.sum(widened * widened, axis=1)
    totals = tuple(
        (jnp.dot(normalized, weight, preferred_element_type=jnp.float32) for weight in weights_all)
    )
    squares, totals = (squares, totals)
    win_proj, key_proj, value_proj, latq_proj, compressed, rope_proj = totals
    row_scale = lax.rsqrt(squares / norm_gain.shape[0] + EPSILON)[:, None]
    offset = lax.axis_index("sp") * tok_rows
    seq_total = tok_rows * lax.axis_size("sp")
    places = (offset + jnp.arange(tok_rows, dtype=jnp.int32)).astype(jnp.float32)
    angles = rotary_angles(places, D_ROPE)
    win_queries = (win_proj * row_scale).astype(jnp.bfloat16)
    key_value = jnp.concatenate(
        [
            (key_proj * row_scale).astype(jnp.bfloat16),
            (value_proj * row_scale).astype(jnp.bfloat16),
        ],
        axis=1,
    )
    padded = padded_2(key_value, (("sp", 0),), WINDOW)
    head_start = lax.axis_index("tp") * sink_logit.shape[0]
    win_out = window_attention(win_queries, padded, sink_logit, offset, seq_total, head_start)
    head_count = lat_query.shape[1] // (UNROTATED_WIDTH + D_ROPE)
    query_all = (latq_proj * row_scale).reshape(tok_rows, head_count, UNROTATED_WIDTH + D_ROPE)
    query_plain = query_all[..., :UNROTATED_WIDTH].astype(jnp.bfloat16)
    query_turned = rotate(query_all[..., UNROTATED_WIDTH:], angles[:, None, :]).astype(jnp.bfloat16)
    latent = (
        compressed
        * lax.rsqrt(jnp.mean(compressed * compressed, axis=1, keepdims=True) + EPSILON)
        * latent_norm_gain[None, :]
    ).astype(jnp.bfloat16)
    key_rotary = rotate(rope_proj * row_scale, angles).astype(jnp.bfloat16)
    attend = partial(latent_step, query_plain=query_plain, query_turned=query_turned)

    def expand(key_block):
        return (
            jnp.dot(key_block[0], key_up_weight, preferred_element_type=jnp.float32).astype(
                jnp.bfloat16
            ),
            jnp.dot(key_block[0], value_up_weight, preferred_element_type=jnp.float32).astype(
                jnp.bfloat16
            ),
            key_block[1],
        )

    _, totals_lat, weighted = over_blocks(
        (
            jnp.full((head_count, tok_rows), -jnp.inf, jnp.float32),
            jnp.zeros((head_count, tok_rows), jnp.float32),
            jnp.zeros((head_count, tok_rows, VALUE_WIDTH), jnp.float32),
        ),
        (
            lax.all_gather(latent, "sp", axis=0, tiled=True),
            lax.all_gather(key_rotary, "sp", axis=0, tiled=True),
        ),
        expand,
        attend,
        2048,
    )
    lat_out = (
        (weighted / totals_lat[..., None])
        .transpose(1, 0, 2)
        .reshape(tok_rows, head_count * VALUE_WIDTH)
    )
    lat_out = lat_out.astype(jnp.bfloat16)
    terms = jnp.dot(win_out, out_win, preferred_element_type=jnp.float32) + jnp.dot(
        lat_out, out_lat, preferred_element_type=jnp.float32
    )
    return lax.psum_scatter(terms.astype(jnp.bfloat16), "tp", scatter_dimension=1, tiled=True)


def dot(a, b, dims=((1,), (0,))):
    return lax.dot_general(a, b, (dims, ((), ())), preferred_element_type=F32)


def whole(count):
    return [pl.BlockSpec(memory_space=pltpu.VMEM)] * count


def scalars(count):
    return [pl.BlockSpec(memory_space=pltpu.SMEM)] * count


def call(body, shapes, smem, operands, flops, mib):
    single = not isinstance(shapes, (list, tuple))
    outs = [shapes] if single else list(shapes)
    result = pl.pallas_call(
        body,
        out_shape=outs,
        in_specs=scalars(len(smem)) + whole(len(operands)),
        out_specs=whole(len(outs)),
        cost_estimate=pl.CostEstimate(
            flops=int(flops),
            bytes_accessed=sum(x.size * x.dtype.itemsize for x in operands),
            transcendentals=0,
        ),
        compiler_params=pltpu.CompilerParams(vmem_limit_bytes=mib * 2**20),
    )(*smem, *operands)
    return result[0] if single else result


def compress_body(part_ref, x_ref, gain_ref, down_ref, rope_ref, norm_ref, own_ref, send_ref):
    rows, half = x_ref.shape
    start = pl.multiple_of(part_ref[0] * half, half)
    wide = x_ref[...].astype(F32)
    normalized = (wide * gain_ref[:, pl.ds(start, half)]).astype(BF16)
    norm_ref[...] = normalized
    compressed = dot(normalized, down_ref[pl.ds(start, half), :])
    rope = dot(normalized, rope_ref[pl.ds(start, half), :])
    squares = jnp.sum(wide * wide, axis=1, keepdims=True)
    high = squares.astype(BF16).astype(F32)
    lane = lax.broadcasted_iota(jnp.int32, (rows, LANES), 1)
    rope = jnp.concatenate([rope, jnp.zeros((rows, LANES - rope.shape[1]), F32)], axis=1)
    width = compressed.shape[1]
    own_ref[:, :width] = compressed
    own_ref[:, width:] = jnp.where(lane == LANES - 1, squares, jnp.where(lane == LANES - 2, 0.0, rope))
    send_ref[:, :width] = compressed.astype(BF16)
    send_ref[:, width:] = jnp.where(
        lane == LANES - 1, high, jnp.where(lane == LANES - 2, squares - high, rope)
    ).astype(BF16)


def turn(vectors, cosines, sines):
    half = vectors.shape[1] // 2
    swapped = jnp.concatenate([vectors[:, half:], vectors[:, :half]], axis=1)
    return vectors * cosines + swapped * sines


def latent_body(own_ref, got_ref, table_ref, gain_ref, block_ref, scale_ref, *, features):
    rows = own_ref.shape[0]
    total = own_ref[...] + got_ref[...].astype(F32)
    width = gain_ref.shape[1]
    compressed = total[:, :width]
    rest = total[:, width:]
    squares = rest[:, LANES - 1 :] + rest[:, LANES - 2 : LANES - 1]
    row_scale = lax.rsqrt(squares / features + EPSILON)
    scale_ref[...] = jnp.broadcast_to(row_scale, scale_ref.shape)
    mean = jnp.mean(compressed * compressed, axis=1, keepdims=True)
    block_ref[:rows] = (compressed * lax.rsqrt(mean + EPSILON) * gain_ref[...]).astype(BF16)
    rope = turn(rest[:, :D_ROPE] * row_scale, table_ref[:, :D_ROPE], table_ref[:, D_ROPE:])
    packed = jnp.concatenate([rope[: rows // 2], rope[rows // 2 :]], axis=1)
    block_ref[rows:] = packed.astype(BF16)


def project_body(
    part_ref, own_ref, got_ref, scale_ref, table_ref, wq_ref, wk_ref, wv_ref, wl_ref, up_ref,
    q_ref, kv_ref, qa_ref, qb_ref,
):
    rows, half = own_ref.shape
    part = part_ref[0]
    mine = pl.multiple_of(part * half, half)
    theirs = pl.multiple_of((1 - part) * half, half)
    own = own_ref[...]
    got = got_ref[...]
    row_scale = scale_ref[:, :1]

    def project(w_ref):
        return (
            dot(own, w_ref[pl.ds(mine, half), :]) + dot(got, w_ref[pl.ds(theirs, half), :])
        ) * row_scale

    width = wk_ref.shape[1]
    kv_ref[:, :width] = project(wk_ref).astype(BF16)
    kv_ref[:, width:] = project(wv_ref).astype(BF16)
    q_ref[...] = (project(wq_ref) * (DH**-0.5 * LOG2E)).astype(BF16)
    queries = project(wl_ref)
    step = UNROTATED_WIDTH + D_ROPE
    scale = step**-0.5 * LOG2E
    row = lax.broadcasted_iota(jnp.int32, (LANES, LANES), 0)
    col = lax.broadcasted_iota(jnp.int32, (LANES, LANES), 1)
    unit = jnp.where(row == col, 1.0, 0.0).astype(BF16)
    blank = jnp.zeros((rows, LANES - D_ROPE), F32)
    chunks = qa_ref.shape[0]
    span = rows // chunks
    lat = up_ref.shape[0]
    for head in range(wl_ref.shape[1] // step):
        plain = queries[:, head * step : head * step + UNROTATED_WIDTH].astype(BF16)
        up = up_ref[:, head * UNROTATED_WIDTH : (head + 1) * UNROTATED_WIDTH]
        low = (dot(up, plain, ((1,), (1,))) * scale).astype(BF16)
        turned = queries[:, head * step + UNROTATED_WIDTH : (head + 1) * step]
        turned = turn(turned, table_ref[:, :D_ROPE], table_ref[:, D_ROPE:]) * scale
        first = jnp.concatenate([turned, blank], axis=1).astype(BF16)
        second = jnp.concatenate([blank, turned], axis=1).astype(BF16)
        first = dot(unit, first, ((1,), (1,))).astype(BF16)
        second = dot(unit, second, ((1,), (1,))).astype(BF16)
        for c in range(chunks):
            cols = slice(head * span, (head + 1) * span)
            rowsl = slice(c * span, (c + 1) * span)
            qa_ref[c, :lat, cols] = low[:, rowsl]
            qb_ref[c, :lat, cols] = low[:, rowsl]
            qa_ref[c, lat:, cols] = first[:, rowsl]
            qb_ref[c, lat:, cols] = second[:, rowsl]


def attend_body(
    place_ref, sink_ref, *refs, groups, chunk, rows,
):
    blocks = refs[:groups]
    (
        qa_ref, qb_ref, q_ref, prev_ref, kv_ref, next_ref, up_ref, ow_ref, ol_ref,
        send_ref, keep_ref, _, cat_ref,
    ) = refs[groups:]
    span = q_ref.shape[0] // qa_ref.shape[0]
    half = rows // 2
    unit = rows + half
    columns = qa_ref.shape[2]
    lat = LANES
    peak = jnp.full((1, columns), MASKED, F32)
    total = jnp.zeros((1, columns), F32)
    weighted = jnp.zeros((lat, columns), F32)
    for block in blocks:
        count = block.shape[0] // unit
        cut = block[...].reshape(count, unit, LANES)
        rope = cut[:, rows:].reshape(count * half, LANES)
        first = cut[:, :half].reshape(count * half, LANES)
        second = cut[:, half:rows].reshape(count * half, LANES)
        for keys, table in ((first, qa_ref), (second, qb_ref)):
            score = dot(jnp.concatenate([keys, rope], axis=1), table[chunk])
            top = jnp.maximum(peak, jnp.max(score, axis=0, keepdims=True))
            factor = jnp.exp2(peak - top)
            weight = jnp.exp2(score - top)
            total = total * factor + jnp.sum(weight, axis=0, keepdims=True)
            weighted = weighted * factor + dot(keys, weight.astype(BF16), ((0,), (0,)))
            peak = top
    mixed = (weighted / total).astype(BF16)

    heads_l = columns // span
    q = q_ref[chunk * span : (chunk + 1) * span, :]
    heads = q.shape[1] // DH
    width = kv_ref.shape[1] // 2
    key_heads = width // DH
    group = heads // key_heads
    padded = jnp.concatenate([prev_ref[...], kv_ref[...], next_ref[...]], axis=0)
    padded = padded[chunk * span : (chunk + 1) * span + 2 * WINDOW]
    offset = place_ref[0]
    key_pos = lax.broadcasted_iota(jnp.int32, (span + 2 * WINDOW, span), 0) - WINDOW
    query_pos = lax.broadcasted_iota(jnp.int32, (span + 2 * WINDOW, span), 1)
    distance = jnp.abs(key_pos - query_pos)
    spot = key_pos + (offset + chunk * span)
    inside = (distance <= WINDOW) & (spot >= 0) & (spot < place_ref[1])
    distance = distance.astype(F32)
    for g in range(key_heads):
        keys = padded[:, g * DH : (g + 1) * DH]
        values = padded[:, width + g * DH : width + (g + 1) * DH]
        for j in range(group):
            head = g * group + j
            score = dot(keys, q[:, head * DH : (head + 1) * DH], ((1,), (1,)))
            score = jnp.where(inside, score - sink_ref[1, head] * distance, MASKED)
            sink = sink_ref[0, head]
            top = jnp.maximum(jnp.max(score, axis=0, keepdims=True), sink)
            weight = jnp.exp2(score - top)
            total = jnp.sum(weight, axis=0, keepdims=True) + jnp.exp2(sink - top)
            out = dot(values, weight.astype(BF16), ((0,), (0,))) / total
            cat_ref[head * DH : (head + 1) * DH, :] = out.astype(BF16)
    base = heads * DH
    for head in range(heads_l):
        up = up_ref[:, head * VALUE_WIDTH : (head + 1) * VALUE_WIDTH]
        out = dot(up, mixed[:, head * span : (head + 1) * span], ((0,), (0,)))
        cat_ref[base + head * VALUE_WIDTH : base + (head + 1) * VALUE_WIDTH, :] = out.astype(BF16)
    keep = keep_ref.shape[1]
    part = place_ref[2]
    mine = pl.multiple_of(part * keep, keep)
    theirs = pl.multiple_of((1 - part) * keep, keep)
    win = cat_ref[:base, :]
    low = cat_ref[base:, :]

    def out_of(start):
        return dot(win, ow_ref[:, pl.ds(start, keep)], ((0,), (0,))) + dot(
            low, ol_ref[:, pl.ds(start, keep)], ((0,), (0,))
        )

    send_ref[...] = out_of(theirs).astype(BF16)
    keep_ref[...] = out_of(mine)


def swap(cells, axis, bit):
    count = lax.axis_size(axis)
    return lax.ppermute(cells, axis, [(i, i ^ bit) for i in range(count)])


def gather(block):
    count = lax.axis_size("sp")
    if count % 4 or count > 16 or count & (count - 1):
        return (lax.all_gather(block, "sp", axis=0, tiled=True),)
    line = [block] + [swap(block, "sp", 4 * k) for k in reversed(range(1, count // 4))]
    near = swap(block, "sp", 2)
    line = jnp.concatenate(line, axis=0)
    far = swap(line[block.shape[0] :], "sp", 2) if count > 4 else line[:0]
    mine = jnp.concatenate([line, near, far], axis=0)
    return (mine, swap(mine, "sp", 1))


def per_device(
    activations,
    norm_gain,
    win_query,
    win_key,
    win_value,
    sink_logit,
    lat_query,
    key_value_down_weight,
    rope_key,
    latent_norm_gain,
    key_up_weight,
    value_up_weight,
    out_win,
    out_lat,
):
    rows, half = activations.shape
    features = norm_gain.shape[0]
    part = lax.axis_index("tp").astype(jnp.int32)
    count = lax.axis_size("sp")
    offset = lax.axis_index("sp").astype(jnp.int32) * rows
    shape = jax.ShapeDtypeStruct

    places = (offset + jnp.arange(rows, dtype=jnp.int32)).astype(F32)
    angles = rotary_angles(places, D_ROPE)
    cosines, sines = jnp.cos(angles), jnp.sin(angles)
    table = jnp.concatenate([cosines, cosines, -sines, sines], axis=1)

    lat = key_value_down_weight.shape[1]
    normalized, own, send = call(
        compress_body,
        [shape((rows, half), BF16), shape((rows, lat + LANES), F32), shape((rows, lat + LANES), BF16)],
        [part[None]],
        [activations, norm_gain[None], key_value_down_weight, rope_key],
        2 * rows * half * 192, 8,
    )
    got = swap(send, "tp", 1)
    other = swap(normalized, "tp", 1)
    block, row_scale = call(
        partial(latent_body, features=features),
        [shape((rows + rows // 2, lat), BF16), shape((rows, LANES), F32)],
        [], [own, got, table, latent_norm_gain[None]],
        1e6, 4,
    )
    blocks = gather(block)

    chunks = rows // WINDOW
    columns = lat_query.shape[1] // (UNROTATED_WIDTH + D_ROPE) * (rows // chunks)
    queries, key_value, table_a, table_b = call(
        project_body,
        [
            shape(win_query.shape[1:] and (rows, win_query.shape[1]), BF16),
            shape((rows, win_key.shape[1] + win_value.shape[1]), BF16),
            shape((chunks, lat + LANES, columns), BF16),
            shape((chunks, lat + LANES, columns), BF16),
        ],
        [part[None]],
        [normalized, other, row_scale, table, win_query, win_key, win_value, lat_query, key_up_weight],
        2 * rows * features * 1792, 20,
    )
    after = lax.ppermute(key_value[rows - WINDOW :], "sp", [(i, i + 1) for i in range(count - 1)])
    before = lax.ppermute(key_value[:WINDOW], "sp", [(i + 1, i) for i in range(count - 1)])

    heads = sink_logit.shape[0]
    head_ids = lax.axis_index("tp") * heads + jnp.arange(heads, dtype=jnp.int32)
    slopes = jnp.exp2(-8.0 * (head_ids + 1).astype(F32) / HEADS_A)
    sinks = jnp.stack([sink_logit, slopes]) * LOG2E
    place = jnp.stack([offset, jnp.int32(rows * count), part])
    kept = []
    for c in range(chunks):
        span = rows // chunks
        send, keep = pl.pallas_call(
            partial(attend_body, groups=len(blocks), chunk=c, rows=rows),
            out_shape=[shape((span, half), BF16), shape((span, half), F32)],
            in_specs=scalars(2) + whole(len(blocks) + 9),
            out_specs=whole(2),
            scratch_shapes=[
                pltpu.VMEM((8, LANES), F32),
                pltpu.VMEM((out_win.shape[0] + out_lat.shape[0], span), BF16),
            ],
            cost_estimate=pl.CostEstimate(flops=3 * 10**9, bytes_accessed=8 * 2**20, transcendentals=0),
            compiler_params=pltpu.CompilerParams(vmem_limit_bytes=32 * 2**20),
        )(
            place, sinks, *blocks, table_a, table_b, queries, after, key_value, before,
            value_up_weight, out_win, out_lat,
        )
        kept.append((keep, swap(send, "tp", 1)))
    return jnp.concatenate([(keep + got.astype(F32)).astype(BF16) for keep, got in kept], axis=0)


def solution(mesh):
    body = per_device if mesh.shape["tp"] == 2 else per_device_wide
    return jax.shard_map(
        body,
        mesh=mesh,
        in_specs=(
            P("sp", "tp"),
            P(),
            P(None, "tp"),
            P(None, "tp"),
            P(None, "tp"),
            P("tp"),
            P(None, "tp"),
            P(),
            P(),
            P(),
            P(None, "tp"),
            P(None, "tp"),
            P("tp", None),
            P("tp", None),
        ),
        out_specs=P("sp", "tp"),
        check_vma=False,
    )
```

```python
from functools import partial

import jax
import jax.numpy as jnp
from jax import lax
from jax.experimental import pallas as pl
from jax.experimental.pallas import tpu as pltpu
from jax.sharding import PartitionSpec as P


HEADS_A = 16
DH = 64
WINDOW = 128
UNROTATED_WIDTH = 128
D_ROPE = 64
VALUE_WIDTH = 128


EPSILON = 1e-06
ROPE_BASE = 10000.0
LOG2E = 1.4426950408889634
LANES = 128
MASKED = -1e30


F32 = jnp.float32
BF16 = jnp.bfloat16


def padded_2(cells, sides, width):
    for axis, dim in sides:
        count = lax.axis_size(axis)
        ends = count - 1
        head = lax.slice_in_dim(cells, 0, width, axis=dim)
        tail = lax.slice_in_dim(cells, cells.shape[dim] - width, cells.shape[dim], axis=dim)
        cells = jnp.concatenate(
            [
                lax.ppermute(tail, axis, [(i, (i + 1) % count) for i in range(ends)]),
                cells,
                lax.ppermute(head, axis, [((i + 1) % count, i) for i in range(ends)]),
            ],
            axis=dim,
        )
    return cells


def rotate(vectors, angles):
    half_width = vectors.shape[-1] // 2
    cosine_table = jnp.cos(angles)
    sine_table = jnp.sin(angles)
    lower_half = vectors[..., :half_width]
    upper_half = vectors[..., half_width:]
    return jnp.concatenate(
        [
            lower_half * cosine_table - upper_half * sine_table,
            lower_half * sine_table + upper_half * cosine_table,
        ],
        axis=-1,
    )


def rotary_angles(places, width):
    frequency = 1.0 / ROPE_BASE ** (jnp.arange(0, width, 2).astype(jnp.float32) / width)
    return places[:, None] * frequency[None, :]


def window_attention(queries, padded, sinks, offset, seq_total, head_start):
    tok_rows = queries.shape[0]
    key_heads = padded.shape[1] // (2 * DH)
    groups = queries.shape[1] // (DH * key_heads)
    key_rows = padded[:, : key_heads * DH].reshape(-1, key_heads, DH)
    value_rows = padded[:, key_heads * DH :].reshape(-1, key_heads, DH)
    grouped = queries.reshape(tok_rows, key_heads, groups, DH)
    scores = jnp.einsum(
        "qhgd,khd->hgqk", grouped, key_rows, preferred_element_type=jnp.float32
    ) * DH ** (-0.5)
    query_pos = offset + jnp.arange(tok_rows, dtype=jnp.int32)
    key_pos = offset - WINDOW + jnp.arange(tok_rows + 2 * WINDOW, dtype=jnp.int32)
    distance = jnp.abs(query_pos[:, None] - key_pos[None, :])
    in_window = (distance <= WINDOW) & (key_pos[None, :] >= 0) & (key_pos[None, :] < seq_total)
    head_ids = head_start + jnp.arange(key_heads * groups, dtype=jnp.int32)
    slopes = jnp.exp2(-8.0 * (head_ids + 1).astype(jnp.float32) / HEADS_A).reshape(
        key_heads, groups
    )
    scores = scores - slopes[:, :, None, None] * distance.astype(jnp.float32)[None, None]
    scores = jnp.where(in_window[None, None], scores, -jnp.inf)
    sink_table = sinks.reshape(key_heads, groups)
    row_peak = jnp.maximum(jnp.max(scores, axis=3), sink_table[:, :, None])
    weights = jnp.exp(scores - row_peak[..., None])
    denominator = jnp.sum(weights, axis=3) + jnp.exp(sink_table[:, :, None] - row_peak)
    blended = jnp.einsum(
        "hgqk,khd->qhgd",
        weights.astype(jnp.bfloat16),
        value_rows,
        preferred_element_type=jnp.float32,
    )
    blended = blended / jnp.transpose(denominator, (2, 0, 1))[..., None]
    return blended.reshape(tok_rows, key_heads * groups * DH).astype(jnp.bfloat16)


def latent_step(running, key_block, query_plain, query_turned):
    row_peak, totals, weighted = running
    keys_plain, values_plain, keys_turned = key_block
    key_count = keys_plain.shape[0]
    head_count = query_plain.shape[1]
    scores = jnp.einsum(
        "qhd,khd->hqk",
        query_plain,
        keys_plain.reshape(key_count, head_count, UNROTATED_WIDTH),
        preferred_element_type=jnp.float32,
    )
    scores = scores + jnp.einsum(
        "qhd,kd->hqk", query_turned, keys_turned, preferred_element_type=jnp.float32
    )
    scores = scores * (UNROTATED_WIDTH + D_ROPE) ** (-0.5)
    new_peak = jnp.maximum(row_peak, jnp.max(scores, axis=2))
    factor = jnp.exp(row_peak - new_peak)
    weights = jnp.exp(scores - new_peak[..., None])
    totals = totals * factor + jnp.sum(weights, axis=2)
    weighted = weighted * factor[..., None] + jnp.einsum(
        "hqk,khd->hqd",
        weights.astype(jnp.bfloat16),
        values_plain.reshape(key_count, head_count, VALUE_WIDTH),
        preferred_element_type=jnp.float32,
    )
    return (new_peak, totals, weighted)


def over_blocks(running, pieces, prepare, attend, block_rows):
    key_count = pieces[0].shape[0]
    stacked = tuple(
        (
            piece_part.reshape((key_count // block_rows, block_rows) + piece_part.shape[1:])
            for piece_part in pieces
        )
    )

    def one_block(state_now, key_block):
        return (attend(state_now, prepare(key_block)), None)

    return lax.scan(one_block, running, stacked)[0]


def per_device_wide(
    activations,
    norm_gain,
    win_query,
    win_key,
    win_value,
    sink_logit,
    lat_query,
    key_value_down_weight,
    rope_key,
    latent_norm_gain,
    key_up_weight,
    value_up_weight,
    out_win,
    out_lat,
):
    tok_rows = activations.shape[0]
    weights_all = (win_query, win_key, win_value, lat_query, key_value_down_weight, rope_key)
    widened = lax.all_gather(activations, "tp", axis=1, tiled=True).astype(jnp.float32)
    normalized = (widened * norm_gain[None, :]).astype(jnp.bfloat16)
    squares = jnp.sum(widened * widened, axis=1)
    totals = tuple(
        (jnp.dot(normalized, weight, preferred_element_type=jnp.float32) for weight in weights_all)
    )
    squares, totals = (squares, totals)
    win_proj, key_proj, value_proj, latq_proj, compressed, rope_proj = totals
    row_scale = lax.rsqrt(squares / norm_gain.shape[0] + EPSILON)[:, None]
    offset = lax.axis_index("sp") * tok_rows
    seq_total = tok_rows * lax.axis_size("sp")
    places = (offset + jnp.arange(tok_rows, dtype=jnp.int32)).astype(jnp.float32)
    angles = rotary_angles(places, D_ROPE)
    win_queries = (win_proj * row_scale).astype(jnp.bfloat16)
    key_value = jnp.concatenate(
        [
            (key_proj * row_scale).astype(jnp.bfloat16),
            (value_proj * row_scale).astype(jnp.bfloat16),
        ],
        axis=1,
    )
    padded = padded_2(key_value, (("sp", 0),), WINDOW)
    head_start = lax.axis_index("tp") * sink_logit.shape[0]
    win_out = window_attention(win_queries, padded, sink_logit, offset, seq_total, head_start)
    head_count = lat_query.shape[1] // (UNROTATED_WIDTH + D_ROPE)
    query_all = (latq_proj * row_scale).reshape(tok_rows, head_count, UNROTATED_WIDTH + D_ROPE)
    query_plain = query_all[..., :UNROTATED_WIDTH].astype(jnp.bfloat16)
    query_turned = rotate(query_all[..., UNROTATED_WIDTH:], angles[:, None, :]).astype(jnp.bfloat16)
    latent = (
        compressed
        * lax.rsqrt(jnp.mean(compressed * compressed, axis=1, keepdims=True) + EPSILON)
        * latent_norm_gain[None, :]
    ).astype(jnp.bfloat16)
    key_rotary = rotate(rope_proj * row_scale, angles).astype(jnp.bfloat16)
    attend = partial(latent_step, query_plain=query_plain, query_turned=query_turned)

    def expand(key_block):
        return (
            jnp.dot(key_block[0], key_up_weight, preferred_element_type=jnp.float32).astype(
                jnp.bfloat16
            ),
            jnp.dot(key_block[0], value_up_weight, preferred_element_type=jnp.float32).astype(
                jnp.bfloat16
            ),
            key_block[1],
        )

    _, totals_lat, weighted = over_blocks(
        (
            jnp.full((head_count, tok_rows), -jnp.inf, jnp.float32),
            jnp.zeros((head_count, tok_rows), jnp.float32),
            jnp.zeros((head_count, tok_rows, VALUE_WIDTH), jnp.float32),
        ),
        (
            lax.all_gather(latent, "sp", axis=0, tiled=True),
            lax.all_gather(key_rotary, "sp", axis=0, tiled=True),
        ),
        expand,
        attend,
        2048,
    )
    lat_out = (
        (weighted / totals_lat[..., None])
        .transpose(1, 0, 2)
        .reshape(tok_rows, head_count * VALUE_WIDTH)
    )
    lat_out = lat_out.astype(jnp.bfloat16)
    terms = jnp.dot(win_out, out_win, preferred_element_type=jnp.float32) + jnp.dot(
        lat_out, out_lat, preferred_element_type=jnp.float32
    )
    return lax.psum_scatter(terms.astype(jnp.bfloat16), "tp", scatter_dimension=1, tiled=True)


def dot(a, b, dims=((1,), (0,))):
    return lax.dot_general(a, b, (dims, ((), ())), preferred_element_type=F32)


def whole(count):
    return [pl.BlockSpec(memory_space=pltpu.VMEM)] * count


def scalars(count):
    return [pl.BlockSpec(memory_space=pltpu.SMEM)] * count


def call(body, shapes, smem, hbm, operands, flops, mib, scratch=()):
    single = not isinstance(shapes, (list, tuple))
    outs = [shapes] if single else list(shapes)
    result = pl.pallas_call(
        body,
        out_shape=outs,
        in_specs=scalars(len(smem))
        + [pl.BlockSpec(memory_space=pltpu.HBM)] * len(hbm)
        + whole(len(operands)),
        out_specs=whole(len(outs)),
        scratch_shapes=list(scratch),
        cost_estimate=pl.CostEstimate(
            flops=int(flops),
            bytes_accessed=sum(x.size * x.dtype.itemsize for x in [*hbm, *operands]),
            transcendentals=0,
        ),
        compiler_params=pltpu.CompilerParams(vmem_limit_bytes=mib * 2**20),
    )(*smem, *[pltpu.with_memory_space_constraint(x, pltpu.HBM) for x in hbm], *operands)
    return result[0] if single else result


def compress_body(
    part_ref, x_hbm, gain_hbm, down_hbm, rope_hbm, norm_ref, own_ref, send_ref,
    x_ref, gain_ref, down_ref, rope_ref, sems,
):
    rows, half = x_hbm.shape
    start = pl.multiple_of(part_ref[0] * half, half)
    copies = [
        pltpu.make_async_copy(x_hbm, x_ref, sems.at[0]),
        pltpu.make_async_copy(gain_hbm.at[:, pl.ds(start, half)], gain_ref, sems.at[3]),
        pltpu.make_async_copy(down_hbm.at[pl.ds(start, half), :], down_ref, sems.at[1]),
        pltpu.make_async_copy(rope_hbm.at[:, pl.ds(start, half)], rope_ref, sems.at[2]),
    ]
    for copy in copies:
        copy.start()
    copies[0].wait()
    copies[1].wait()
    wide = x_ref[...].astype(F32)
    normalized = (wide * gain_ref[...]).astype(BF16)
    norm_ref[...] = normalized
    squares = jnp.sum(wide * wide, axis=1, keepdims=True)
    copies[2].wait()
    compressed = dot(normalized, down_ref[...])
    copies[3].wait()
    rope = dot(normalized, rope_ref[...], ((1,), (1,)))
    high = squares.astype(BF16).astype(F32)
    lane = lax.broadcasted_iota(jnp.int32, (rows, LANES), 1)
    rope = jnp.concatenate([rope, jnp.zeros((rows, LANES - rope.shape[1]), F32)], axis=1)
    width = compressed.shape[1]
    own_ref[:, :width] = compressed
    own_ref[:, width:] = jnp.where(lane == LANES - 1, squares, jnp.where(lane == LANES - 2, 0.0, rope))
    send_ref[:, :width] = compressed.astype(BF16)
    send_ref[:, width:] = jnp.where(
        lane == LANES - 1, high, jnp.where(lane == LANES - 2, squares - high, rope)
    ).astype(BF16)


def turn(vectors, cosines, sines):
    half = vectors.shape[1] // 2
    swapped = jnp.concatenate([vectors[:, half:], vectors[:, :half]], axis=1)
    return vectors * cosines + swapped * sines


def latent_body(own_ref, got_ref, table_ref, gain_ref, block_ref, scale_ref, *, features):
    rows = own_ref.shape[0]
    total = own_ref[...] + got_ref[...].astype(F32)
    width = gain_ref.shape[1]
    compressed = total[:, :width]
    rest = total[:, width:]
    squares = rest[:, LANES - 1 :] + rest[:, LANES - 2 : LANES - 1]
    row_scale = lax.rsqrt(squares / features + EPSILON)
    scale_ref[...] = jnp.broadcast_to(row_scale, scale_ref.shape)
    mean = jnp.mean(compressed * compressed, axis=1, keepdims=True)
    block_ref[:rows] = (compressed * lax.rsqrt(mean + EPSILON) * gain_ref[...]).astype(BF16)
    rope = turn(rest[:, :D_ROPE] * row_scale, table_ref[:, :D_ROPE], table_ref[:, D_ROPE:])
    packed = jnp.concatenate([rope[: rows // 2], rope[rows // 2 :]], axis=1)
    block_ref[rows:] = packed.astype(BF16)


def own_body(part_ref, *refs, count):
    weights = refs[:count]
    own_ref = refs[count]
    sums = refs[count + 1 : 2 * count + 1]
    rests = refs[2 * count + 1 : 3 * count + 1]
    mines = refs[3 * count + 1 : 4 * count + 1]
    sems = refs[-1]
    half = own_ref.shape[1]
    part = part_ref[0]
    mine = pl.multiple_of(part * half, half)
    theirs = pl.multiple_of((1 - part) * half, half)
    first = [
        pltpu.make_async_copy(w.at[pl.ds(mine, half), :], m, sems.at[0, i])
        for i, (w, m) in enumerate(zip(weights, mines))
    ]
    second = [
        pltpu.make_async_copy(w.at[pl.ds(theirs, half), :], r, sems.at[1, i])
        for i, (w, r) in enumerate(zip(weights, rests))
    ]
    for copy in first + second:
        copy.start()
    own = own_ref[...]
    for copy, mine_ref, sum_ref in zip(first, mines, sums):
        copy.wait()
        sum_ref[...] = dot(own, mine_ref[...])
    for copy in second:
        copy.wait()


def project_body(
    got_ref, scale_ref, table_ref, sk_ref, sv_ref, sq_ref, sl_ref, wk_ref, wv_ref, wq_ref, wl_ref,
    up_ref, q_ref, kv_ref, qa_ref, qb_ref,
):
    got = got_ref[...]
    rows = got.shape[0]
    row_scale = scale_ref[:, :1]

    def project(sum_ref, w_ref):
        return (sum_ref[...] + dot(got, w_ref[...])) * row_scale

    width = wk_ref.shape[1]
    kv_ref[:, :width] = project(sk_ref, wk_ref).astype(BF16)
    kv_ref[:, width:] = project(sv_ref, wv_ref).astype(BF16)
    win = (project(sq_ref, wq_ref) * (DH**-0.5 * LOG2E)).astype(BF16)
    queries = project(sl_ref, wl_ref)
    step = UNROTATED_WIDTH + D_ROPE
    scale = step**-0.5 * LOG2E
    row = lax.broadcasted_iota(jnp.int32, (LANES, LANES), 0)
    col = lax.broadcasted_iota(jnp.int32, (LANES, LANES), 1)
    unit = jnp.where(row == col, 1.0, 0.0).astype(BF16)
    blank = jnp.zeros((rows, LANES - D_ROPE), F32)
    chunks = qa_ref.shape[0]
    span = rows // chunks
    shared = LANES // DH
    group = win.shape[1] // width
    for g in range(width // DH):
        pair = dot(unit, win[:, g * group * DH : (g + 1) * group * DH], ((1,), (1,))).astype(BF16)
        spot = g % shared * DH
        for c in range(chunks):
            q_ref[c, g] = jnp.zeros(q_ref.shape[2:], BF16)
            for j in range(group):
                q_ref[c, g, spot : spot + DH, j * span : (j + 1) * span] = pair[
                    j * DH : (j + 1) * DH, c * span : (c + 1) * span
                ]
    lat = up_ref.shape[0]
    for head in range(wl_ref.shape[1] // step):
        plain = queries[:, head * step : head * step + UNROTATED_WIDTH].astype(BF16)
        up = up_ref[:, head * UNROTATED_WIDTH : (head + 1) * UNROTATED_WIDTH]
        low = (dot(up, plain, ((1,), (1,))) * scale).astype(BF16)
        turned = queries[:, head * step + UNROTATED_WIDTH : (head + 1) * step]
        turned = turn(turned, table_ref[:, :D_ROPE], table_ref[:, D_ROPE:]) * scale
        first = jnp.concatenate([turned, blank], axis=1).astype(BF16)
        second = jnp.concatenate([blank, turned], axis=1).astype(BF16)
        first = dot(unit, first, ((1,), (1,))).astype(BF16)
        second = dot(unit, second, ((1,), (1,))).astype(BF16)
        for c in range(chunks):
            cols = slice(head * span, (head + 1) * span)
            rowsl = slice(c * span, (c + 1) * span)
            qa_ref[c, :lat, cols] = low[:, rowsl]
            qb_ref[c, :lat, cols] = low[:, rowsl]
            qa_ref[c, lat:, cols] = first[:, rowsl]
            qb_ref[c, lat:, cols] = second[:, rowsl]


def attend_body(*refs, groups, chunk, rows):
    qa_ref, qb_ref, mixed_ref = refs[-3:]
    half = rows // 2
    columns = qa_ref.shape[2]
    steps = []
    start = 0
    for size in groups:
        steps += [(refs[start : start + size], 0, qa_ref), (refs[start : start + size], 1, qb_ref)]
        start += size

    def keys_of(step):
        blocks, part, _ = step
        return jnp.concatenate([b[part * half : (part + 1) * half] for b in blocks], axis=0)

    def score_of(step):
        rope = jnp.concatenate([b[rows : rows + half] for b in step[0]], axis=0)
        return dot(jnp.concatenate([keys_of(step), rope], axis=1), step[2][chunk])

    peak = jnp.full((1, columns), MASKED, F32)
    total = jnp.zeros((8, columns), F32)
    weighted = jnp.zeros((LANES, columns), F32)
    coming = score_of(steps[0])
    for i, step in enumerate(steps):
        score = coming
        if i + 1 < len(steps):
            coming = score_of(steps[i + 1])
        top = jnp.maximum(peak, jnp.max(score, axis=0, keepdims=True))
        factor = jnp.exp2(peak - top)
        weight = jnp.exp2(score - top)
        total = total * factor + jnp.sum(weight.reshape(-1, 8, columns), axis=0)
        weighted = weighted * factor + dot(keys_of(step), weight.astype(BF16), ((0,), (0,)))
        peak = top
    mixed_ref[...] = (weighted / jnp.sum(total, axis=0, keepdims=True)).astype(BF16)


def finish_body(
    place_ref, sink_ref, mixed_ref, q_ref, prev_ref, kv_ref, next_ref, up_ref, ow_ref, ol_ref,
    send_ref, keep_ref, cat_ref, *, chunk,
):
    span, columns = send_ref.shape[0], mixed_ref.shape[1]
    mixed = mixed_ref[...]
    heads_l = columns // span
    _, key_heads, lanes, width = q_ref.shape
    group = width // span
    shared = lanes // DH
    own_rows = kv_ref.shape[0]
    pieces = []
    if chunk == 0:
        pieces = [prev_ref[...]]
    low_row = max(chunk * span - WINDOW, 0)
    high_row = min((chunk + 1) * span + WINDOW, own_rows)
    pieces.append(kv_ref[low_row:high_row])
    if (chunk + 1) * span == own_rows:
        pieces.append(next_ref[...])
    padded = jnp.concatenate(pieces, axis=0)
    offset = place_ref[0]
    key_pos = lax.broadcasted_iota(jnp.int32, (span + 2 * WINDOW, span), 0) - WINDOW
    query_pos = lax.broadcasted_iota(jnp.int32, (span + 2 * WINDOW, span), 1)
    distance = jnp.abs(key_pos - query_pos)
    spot = key_pos + (offset + chunk * span)
    inside = (distance <= WINDOW) & (spot >= 0) & (spot < place_ref[1])
    distance = jnp.where(inside, distance.astype(F32), -MASKED)
    distance = jnp.concatenate([distance] * group, axis=1)
    values_at = kv_ref.shape[1] // 2

    def spread(row, g):
        return jnp.concatenate(
            [jnp.full((1, span), sink_ref[row, g * group + j], F32) for j in range(group)], axis=1
        )

    def score_of(g):
        at = g // shared * lanes
        return dot(padded[:, at : at + lanes], q_ref[chunk, g])

    coming = score_of(0)
    for g in range(key_heads):
        score = coming
        if g + 1 < key_heads:
            coming = score_of(g + 1)
        at = values_at + g // shared * lanes
        score = score - spread(1, g) * distance
        sink = spread(0, g)
        top = jnp.maximum(jnp.max(score, axis=0, keepdims=True), sink)
        weight = jnp.exp2(score - top)
        total = jnp.sum(weight, axis=0, keepdims=True) + jnp.exp2(sink - top)
        out = dot(padded[:, at : at + lanes], weight.astype(BF16), ((0,), (0,)))
        row = g % shared * DH
        out = (out[row : row + DH] / total).astype(BF16)
        for j in range(group):
            head = g * group + j
            cat_ref[head * DH : (head + 1) * DH, :] = out[:, j * span : (j + 1) * span]
    base = key_heads * group * DH
    for head in range(heads_l):
        up = up_ref[:, head * VALUE_WIDTH : (head + 1) * VALUE_WIDTH]
        out = dot(up, mixed[:, head * span : (head + 1) * span], ((0,), (0,)))
        cat_ref[base + head * VALUE_WIDTH : base + (head + 1) * VALUE_WIDTH, :] = out.astype(BF16)
    keep = keep_ref.shape[1]
    win = cat_ref[:base, :]
    low = cat_ref[base:, :]

    def out_of(start):
        return dot(win, ow_ref[:, start : start + keep], ((0,), (0,))) + dot(
            low, ol_ref[:, start : start + keep], ((0,), (0,))
        )

    first = out_of(0)
    second = out_of(keep)
    lower = place_ref[2] == 0
    send_ref[...] = jnp.where(lower, second, first).astype(BF16)
    keep_ref[...] = jnp.where(lower, first, second)


def swap(cells, axis, bit):
    count = lax.axis_size(axis)
    return lax.ppermute(cells, axis, [(i, i ^ bit) for i in range(count)])


def gather(block):
    count = lax.axis_size("sp")
    if count % 4 or count > 16 or count & (count - 1):
        return [[block_of] for block_of in jnp.split(lax.all_gather(block, "sp", axis=0, tiled=True), count)]
    line = [block] + [swap(block, "sp", 4 * k) for k in range(1, count // 4)]
    mine = line + [swap(b, "sp", 2) for b in line]
    return [mine, [swap(b, "sp", 1) for b in mine]]


def per_device(
    activations,
    norm_gain,
    win_query,
    win_key,
    win_value,
    sink_logit,
    lat_query,
    key_value_down_weight,
    rope_key,
    latent_norm_gain,
    key_up_weight,
    value_up_weight,
    out_win,
    out_lat,
):
    rows, half = activations.shape
    features = norm_gain.shape[0]
    part = lax.axis_index("tp").astype(jnp.int32)
    count = lax.axis_size("sp")
    offset = lax.axis_index("sp").astype(jnp.int32) * rows
    shape = jax.ShapeDtypeStruct

    places = (offset + jnp.arange(rows, dtype=jnp.int32)).astype(F32)
    angles = rotary_angles(places, D_ROPE)
    cosines, sines = jnp.cos(angles), jnp.sin(angles)
    table = jnp.concatenate([cosines, cosines, -sines, sines], axis=1)

    lat = key_value_down_weight.shape[1]
    normalized, own, send = call(
        compress_body,
        [shape((rows, half), BF16), shape((rows, lat + LANES), F32), shape((rows, lat + LANES), BF16)],
        [part[None]], [activations, norm_gain[None], key_value_down_weight, rope_key.T], [],
        2 * rows * half * 192, 8,
        [
            pltpu.VMEM((rows, half), BF16),
            pltpu.VMEM((1, half), F32),
            pltpu.VMEM((half, lat), BF16),
            pltpu.VMEM((rope_key.shape[1], half), BF16),
            pltpu.SemaphoreType.DMA((4,)),
        ],
    )
    got = swap(send, "tp", 1)
    other = swap(normalized, "tp", 1)
    weights = [win_key, win_value, win_query, lat_query]
    partial_sums = call(
        partial(own_body, count=len(weights)),
        [shape((rows, w.shape[1]), F32) for w in weights]
        + [shape((half, w.shape[1]), BF16) for w in weights],
        [part[None]], weights, [normalized],
        2 * rows * half * 1792, 16,
        [pltpu.VMEM((half, w.shape[1]), BF16) for w in weights]
        + [pltpu.SemaphoreType.DMA((2, len(weights)))],
    )
    block, row_scale = call(
        partial(latent_body, features=features),
        [shape((rows + rows // 2, lat), BF16), shape((rows, LANES), F32)],
        [], [], [own, got, table, latent_norm_gain[None]],
        1e6, 4,
    )
    groups = gather(block)

    chunks = rows // WINDOW
    span = rows // chunks
    group = win_query.shape[1] // win_key.shape[1]
    columns = lat_query.shape[1] // (UNROTATED_WIDTH + D_ROPE) * (rows // chunks)
    queries, key_value, table_a, table_b = call(
        project_body,
        [
            shape((chunks, win_key.shape[1] // DH, LANES, group * span), BF16),
            shape((rows, win_key.shape[1] + win_value.shape[1]), BF16),
            shape((chunks, lat + LANES, columns), BF16),
            shape((chunks, lat + LANES, columns), BF16),
        ],
        [], [],
        [other, row_scale, table, *partial_sums, key_up_weight],
        2 * rows * half * 1792, 16,
    )
    after = lax.ppermute(key_value[rows - WINDOW :], "sp", [(i, i + 1) for i in range(count - 1)])
    before = lax.ppermute(key_value[:WINDOW], "sp", [(i + 1, i) for i in range(count - 1)])

    heads = sink_logit.shape[0]
    head_ids = lax.axis_index("tp") * heads + jnp.arange(heads, dtype=jnp.int32)
    slopes = jnp.exp2(-8.0 * (head_ids + 1).astype(F32) / HEADS_A)
    sinks = jnp.stack([sink_logit, slopes]) * LOG2E
    place = jnp.stack([offset, jnp.int32(rows * count), part])
    kept = []
    flat = [b for group in groups for b in group]
    for c in range(chunks):
        mixed = call(
            partial(attend_body, groups=[len(g) for g in groups], chunk=c, rows=rows),
            shape((lat, columns), BF16), [], [], [*flat, table_a, table_b], 3e9, 32,
        )
        send, keep = call(
            partial(finish_body, chunk=c),
            [shape((span, half), BF16), shape((span, half), F32)],
            [place, sinks], [],
            [mixed, queries, after, key_value, before, value_up_weight, out_win, out_lat],
            1e9, 16,
            [pltpu.VMEM((out_win.shape[0] + out_lat.shape[0], span), BF16)],
        )
        kept.append((keep, swap(send, "tp", 1)))
    return jnp.concatenate([(keep + got.astype(F32)).astype(BF16) for keep, got in kept], axis=0)


def solution(mesh):
    narrow = mesh.shape["tp"] == 2
    body = per_device if narrow else per_device_wide
    return jax.shard_map(
        body,
        mesh=mesh,
        in_specs=(
            P("sp", "tp"),
            P(),
            P(None, "tp"),
            P(None, "tp"),
            P(None, "tp"),
            P("tp"),
            P(None, "tp"),
            P(),
            P(),
            P(),
            P(None, "tp"),
            P(None, "tp"),
            P("tp", None),
            P("tp", None),
        ),
        out_specs=P("sp", "tp"),
        check_vma=False,
    )
```

```python
from functools import partial

import jax
import jax.numpy as jnp
from jax import lax
from jax.experimental import pallas as pl
from jax.experimental.pallas import tpu as pltpu
from jax.sharding import PartitionSpec as P


HEADS_A = 16
DH = 64
WINDOW = 128
UNROTATED_WIDTH = 128
D_ROPE = 64
VALUE_WIDTH = 128


EPSILON = 1e-06
ROPE_BASE = 10000.0
LOG2E = 1.4426950408889634
LANES = 128
MASKED = -1e30


F32 = jnp.float32
BF16 = jnp.bfloat16


def padded_2(cells, sides, width):
    for axis, dim in sides:
        count = lax.axis_size(axis)
        ends = count - 1
        head = lax.slice_in_dim(cells, 0, width, axis=dim)
        tail = lax.slice_in_dim(cells, cells.shape[dim] - width, cells.shape[dim], axis=dim)
        cells = jnp.concatenate(
            [
                lax.ppermute(tail, axis, [(i, (i + 1) % count) for i in range(ends)]),
                cells,
                lax.ppermute(head, axis, [((i + 1) % count, i) for i in range(ends)]),
            ],
            axis=dim,
        )
    return cells


def rotate(vectors, angles):
    half_width = vectors.shape[-1] // 2
    cosine_table = jnp.cos(angles)
    sine_table = jnp.sin(angles)
    lower_half = vectors[..., :half_width]
    upper_half = vectors[..., half_width:]
    return jnp.concatenate(
        [
            lower_half * cosine_table - upper_half * sine_table,
            lower_half * sine_table + upper_half * cosine_table,
        ],
        axis=-1,
    )


def rotary_angles(places, width):
    frequency = 1.0 / ROPE_BASE ** (jnp.arange(0, width, 2).astype(jnp.float32) / width)
    return places[:, None] * frequency[None, :]


def window_attention(queries, padded, sinks, offset, seq_total, head_start):
    tok_rows = queries.shape[0]
    key_heads = padded.shape[1] // (2 * DH)
    groups = queries.shape[1] // (DH * key_heads)
    key_rows = padded[:, : key_heads * DH].reshape(-1, key_heads, DH)
    value_rows = padded[:, key_heads * DH :].reshape(-1, key_heads, DH)
    grouped = queries.reshape(tok_rows, key_heads, groups, DH)
    scores = jnp.einsum(
        "qhgd,khd->hgqk", grouped, key_rows, preferred_element_type=jnp.float32
    ) * DH ** (-0.5)
    query_pos = offset + jnp.arange(tok_rows, dtype=jnp.int32)
    key_pos = offset - WINDOW + jnp.arange(tok_rows + 2 * WINDOW, dtype=jnp.int32)
    distance = jnp.abs(query_pos[:, None] - key_pos[None, :])
    in_window = (distance <= WINDOW) & (key_pos[None, :] >= 0) & (key_pos[None, :] < seq_total)
    head_ids = head_start + jnp.arange(key_heads * groups, dtype=jnp.int32)
    slopes = jnp.exp2(-8.0 * (head_ids + 1).astype(jnp.float32) / HEADS_A).reshape(
        key_heads, groups
    )
    scores = scores - slopes[:, :, None, None] * distance.astype(jnp.float32)[None, None]
    scores = jnp.where(in_window[None, None], scores, -jnp.inf)
    sink_table = sinks.reshape(key_heads, groups)
    row_peak = jnp.maximum(jnp.max(scores, axis=3), sink_table[:, :, None])
    weights = jnp.exp(scores - row_peak[..., None])
    denominator = jnp.sum(weights, axis=3) + jnp.exp(sink_table[:, :, None] - row_peak)
    blended = jnp.einsum(
        "hgqk,khd->qhgd",
        weights.astype(jnp.bfloat16),
        value_rows,
        preferred_element_type=jnp.float32,
    )
    blended = blended / jnp.transpose(denominator, (2, 0, 1))[..., None]
    return blended.reshape(tok_rows, key_heads * groups * DH).astype(jnp.bfloat16)


def latent_step(running, key_block, query_plain, query_turned):
    row_peak, totals, weighted = running
    keys_plain, values_plain, keys_turned = key_block
    key_count = keys_plain.shape[0]
    head_count = query_plain.shape[1]
    scores = jnp.einsum(
        "qhd,khd->hqk",
        query_plain,
        keys_plain.reshape(key_count, head_count, UNROTATED_WIDTH),
        preferred_element_type=jnp.float32,
    )
    scores = scores + jnp.einsum(
        "qhd,kd->hqk", query_turned, keys_turned, preferred_element_type=jnp.float32
    )
    scores = scores * (UNROTATED_WIDTH + D_ROPE) ** (-0.5)
    new_peak = jnp.maximum(row_peak, jnp.max(scores, axis=2))
    factor = jnp.exp(row_peak - new_peak)
    weights = jnp.exp(scores - new_peak[..., None])
    totals = totals * factor + jnp.sum(weights, axis=2)
    weighted = weighted * factor[..., None] + jnp.einsum(
        "hqk,khd->hqd",
        weights.astype(jnp.bfloat16),
        values_plain.reshape(key_count, head_count, VALUE_WIDTH),
        preferred_element_type=jnp.float32,
    )
    return (new_peak, totals, weighted)


def over_blocks(running, pieces, prepare, attend, block_rows):
    key_count = pieces[0].shape[0]
    stacked = tuple(
        (
            piece_part.reshape((key_count // block_rows, block_rows) + piece_part.shape[1:])
            for piece_part in pieces
        )
    )

    def one_block(state_now, key_block):
        return (attend(state_now, prepare(key_block)), None)

    return lax.scan(one_block, running, stacked)[0]


def per_device_wide(
    activations,
    norm_gain,
    win_query,
    win_key,
    win_value,
    sink_logit,
    lat_query,
    key_value_down_weight,
    rope_key,
    latent_norm_gain,
    key_up_weight,
    value_up_weight,
    out_win,
    out_lat,
):
    tok_rows = activations.shape[0]
    weights_all = (win_query, win_key, win_value, lat_query, key_value_down_weight, rope_key)
    widened = lax.all_gather(activations, "tp", axis=1, tiled=True).astype(jnp.float32)
    normalized = (widened * norm_gain[None, :]).astype(jnp.bfloat16)
    squares = jnp.sum(widened * widened, axis=1)
    totals = tuple(
        (jnp.dot(normalized, weight, preferred_element_type=jnp.float32) for weight in weights_all)
    )
    squares, totals = (squares, totals)
    win_proj, key_proj, value_proj, latq_proj, compressed, rope_proj = totals
    row_scale = lax.rsqrt(squares / norm_gain.shape[0] + EPSILON)[:, None]
    offset = lax.axis_index("sp") * tok_rows
    seq_total = tok_rows * lax.axis_size("sp")
    places = (offset + jnp.arange(tok_rows, dtype=jnp.int32)).astype(jnp.float32)
    angles = rotary_angles(places, D_ROPE)
    win_queries = (win_proj * row_scale).astype(jnp.bfloat16)
    key_value = jnp.concatenate(
        [
            (key_proj * row_scale).astype(jnp.bfloat16),
            (value_proj * row_scale).astype(jnp.bfloat16),
        ],
        axis=1,
    )
    padded = padded_2(key_value, (("sp", 0),), WINDOW)
    head_start = lax.axis_index("tp") * sink_logit.shape[0]
    win_out = window_attention(win_queries, padded, sink_logit, offset, seq_total, head_start)
    head_count = lat_query.shape[1] // (UNROTATED_WIDTH + D_ROPE)
    query_all = (latq_proj * row_scale).reshape(tok_rows, head_count, UNROTATED_WIDTH + D_ROPE)
    query_plain = query_all[..., :UNROTATED_WIDTH].astype(jnp.bfloat16)
    query_turned = rotate(query_all[..., UNROTATED_WIDTH:], angles[:, None, :]).astype(jnp.bfloat16)
    latent = (
        compressed
        * lax.rsqrt(jnp.mean(compressed * compressed, axis=1, keepdims=True) + EPSILON)
        * latent_norm_gain[None, :]
    ).astype(jnp.bfloat16)
    key_rotary = rotate(rope_proj * row_scale, angles).astype(jnp.bfloat16)
    attend = partial(latent_step, query_plain=query_plain, query_turned=query_turned)

    def expand(key_block):
        return (
            jnp.dot(key_block[0], key_up_weight, preferred_element_type=jnp.float32).astype(
                jnp.bfloat16
            ),
            jnp.dot(key_block[0], value_up_weight, preferred_element_type=jnp.float32).astype(
                jnp.bfloat16
            ),
            key_block[1],
        )

    _, totals_lat, weighted = over_blocks(
        (
            jnp.full((head_count, tok_rows), -jnp.inf, jnp.float32),
            jnp.zeros((head_count, tok_rows), jnp.float32),
            jnp.zeros((head_count, tok_rows, VALUE_WIDTH), jnp.float32),
        ),
        (
            lax.all_gather(latent, "sp", axis=0, tiled=True),
            lax.all_gather(key_rotary, "sp", axis=0, tiled=True),
        ),
        expand,
        attend,
        2048,
    )
    lat_out = (
        (weighted / totals_lat[..., None])
        .transpose(1, 0, 2)
        .reshape(tok_rows, head_count * VALUE_WIDTH)
    )
    lat_out = lat_out.astype(jnp.bfloat16)
    terms = jnp.dot(win_out, out_win, preferred_element_type=jnp.float32) + jnp.dot(
        lat_out, out_lat, preferred_element_type=jnp.float32
    )
    return lax.psum_scatter(terms.astype(jnp.bfloat16), "tp", scatter_dimension=1, tiled=True)


def dot(a, b, dims=((1,), (0,))):
    return lax.dot_general(a, b, (dims, ((), ())), preferred_element_type=F32)


def whole(count):
    return [pl.BlockSpec(memory_space=pltpu.VMEM)] * count


def scalars(count):
    return [pl.BlockSpec(memory_space=pltpu.SMEM)] * count


def call(body, shapes, smem, hbm, operands, flops, mib, scratch=()):
    single = not isinstance(shapes, (list, tuple))
    outs = [shapes] if single else list(shapes)
    result = pl.pallas_call(
        body,
        out_shape=outs,
        in_specs=scalars(len(smem))
        + [pl.BlockSpec(memory_space=pltpu.HBM)] * len(hbm)
        + whole(len(operands)),
        out_specs=whole(len(outs)),
        scratch_shapes=list(scratch),
        cost_estimate=pl.CostEstimate(
            flops=int(flops),
            bytes_accessed=sum(x.size * x.dtype.itemsize for x in [*hbm, *operands]),
            transcendentals=0,
        ),
        compiler_params=pltpu.CompilerParams(vmem_limit_bytes=mib * 2**20),
    )(*smem, *[pltpu.with_memory_space_constraint(x, pltpu.HBM) for x in hbm], *operands)
    return result[0] if single else result


def compress_body(
    offset_ref, part_ref, parity_ref, x_hbm, gain_hbm, down_hbm, rope_hbm, norm_ref, own_ref, send_ref,
    x_ref, gain_ref, down_ref, rope_ref, sems,
):
    rows, half = x_hbm.shape
    del offset_ref, parity_ref
    start = pl.multiple_of(part_ref[0] * half, half)
    copies = [
        pltpu.make_async_copy(x_hbm, x_ref, sems.at[0]),
        pltpu.make_async_copy(gain_hbm.at[:, pl.ds(start, half)], gain_ref, sems.at[3]),
        pltpu.make_async_copy(down_hbm.at[pl.ds(start, half), :], down_ref, sems.at[1]),
        pltpu.make_async_copy(rope_hbm.at[:, pl.ds(start, half)], rope_ref, sems.at[2]),
    ]
    for copy in copies:
        copy.start()
    copies[0].wait()
    copies[1].wait()
    wide = x_ref[...].astype(F32)
    normalized = (wide * gain_ref[...]).astype(BF16)
    norm_ref[...] = normalized
    squares = jnp.sum(wide * wide, axis=1, keepdims=True)
    copies[2].wait()
    compressed = dot(normalized, down_ref[...])
    copies[3].wait()
    rope = dot(normalized, rope_ref[...], ((1,), (1,)))
    high = squares.astype(BF16).astype(F32)
    lane = lax.broadcasted_iota(jnp.int32, (rows, LANES), 1)
    rope = jnp.concatenate([rope, jnp.zeros((rows, LANES - rope.shape[1]), F32)], axis=1)
    width = compressed.shape[1]
    own_ref[:, :width] = compressed
    own_ref[:, width:] = jnp.where(lane == LANES - 1, squares, jnp.where(lane == LANES - 2, 0.0, rope))
    send_ref[:, :width] = compressed.astype(BF16)
    send_ref[:, width:] = jnp.where(
        lane == LANES - 1, high, jnp.where(lane == LANES - 2, squares - high, rope)
    ).astype(BF16)


def turn(vectors, cosines, sines):
    half = vectors.shape[1] // 2
    swapped = jnp.concatenate([vectors[:, half:], vectors[:, :half]], axis=1)
    return vectors * cosines + swapped * sines


def latent_body(own_ref, got_ref, table_ref, gain_ref, block_ref, scale_ref, *, features):
    rows = own_ref.shape[0]
    total = own_ref[...] + got_ref[...].astype(F32)
    width = gain_ref.shape[1]
    compressed = total[:, :width]
    rest = total[:, width:]
    squares = rest[:, LANES - 1 :] + rest[:, LANES - 2 : LANES - 1]
    row_scale = lax.rsqrt(squares / features + EPSILON)
    scale_ref[...] = jnp.broadcast_to(row_scale, scale_ref.shape)
    mean = jnp.mean(compressed * compressed, axis=1, keepdims=True)
    block_ref[:rows] = (compressed * lax.rsqrt(mean + EPSILON) * gain_ref[...]).astype(BF16)
    rope = turn(rest[:, :D_ROPE] * row_scale, table_ref[:, :D_ROPE], table_ref[:, D_ROPE:])
    packed = jnp.concatenate([rope[: rows // 2], rope[rows // 2 :]], axis=1)
    block_ref[rows:] = packed.astype(BF16)


def own_body(part_ref, *refs, count):
    weights = refs[:count]
    own_ref = refs[count]
    sums = refs[count + 1 : 2 * count + 1]
    rests = refs[2 * count + 1 : 3 * count + 1]
    mines = refs[3 * count + 1 : 4 * count + 1]
    sems = refs[-1]
    half = own_ref.shape[1]
    part = part_ref[0]
    mine = pl.multiple_of(part * half, half)
    theirs = pl.multiple_of((1 - part) * half, half)
    first = [
        pltpu.make_async_copy(w.at[pl.ds(mine, half), :], m, sems.at[0, i])
        for i, (w, m) in enumerate(zip(weights, mines))
    ]
    second = [
        pltpu.make_async_copy(w.at[pl.ds(theirs, half), :], r, sems.at[1, i])
        for i, (w, r) in enumerate(zip(weights, rests))
    ]
    for copy in first + second:
        copy.start()
    own = own_ref[...]
    for copy, mine_ref, sum_ref in zip(first, mines, sums):
        copy.wait()
        sum_ref[...] = dot(own, mine_ref[...])
    for copy in second:
        copy.wait()


def project_body(
    parity_ref, got_ref, scale_ref, table_ref, sk_ref, sv_ref, sq_ref, sl_ref, wk_ref, wv_ref, wq_ref, wl_ref,
    up_ref, q_ref, kv_ref, in_ref, out_ref, qa_ref, qb_ref,
):
    got = got_ref[...]
    rows = got.shape[0]
    row_scale = scale_ref[:, :1]

    def project(sum_ref, w_ref):
        return (sum_ref[...] + dot(got, w_ref[...])) * row_scale

    width = wk_ref.shape[1]
    kv_ref[:, :width] = project(sk_ref, wk_ref).astype(BF16)
    kv_ref[:, width:] = project(sv_ref, wv_ref).astype(BF16)
    even = parity_ref[0] == 0
    head = kv_ref[:WINDOW]
    tail = kv_ref[rows - WINDOW :]
    in_ref[...] = jnp.where(even, tail, head)
    out_ref[...] = jnp.where(even, head, tail)
    win = (project(sq_ref, wq_ref) * (DH**-0.5 * LOG2E)).astype(BF16)
    queries = project(sl_ref, wl_ref)
    step = UNROTATED_WIDTH + D_ROPE
    scale = step**-0.5 * LOG2E
    row = lax.broadcasted_iota(jnp.int32, (LANES, LANES), 0)
    col = lax.broadcasted_iota(jnp.int32, (LANES, LANES), 1)
    unit = jnp.where(row == col, 1.0, 0.0).astype(BF16)
    blank = jnp.zeros((rows, LANES - D_ROPE), F32)
    chunks = qa_ref.shape[0]
    span = rows // chunks
    shared = LANES // DH
    group = win.shape[1] // width
    for g in range(width // DH):
        pair = dot(unit, win[:, g * group * DH : (g + 1) * group * DH], ((1,), (1,))).astype(BF16)
        spot = g % shared * DH
        for c in range(chunks):
            q_ref[c, g] = jnp.zeros(q_ref.shape[2:], BF16)
            for j in range(group):
                q_ref[c, g, spot : spot + DH, j * span : (j + 1) * span] = pair[
                    j * DH : (j + 1) * DH, c * span : (c + 1) * span
                ]
    lat = up_ref.shape[0]
    for head in range(wl_ref.shape[1] // step):
        plain = queries[:, head * step : head * step + UNROTATED_WIDTH].astype(BF16)
        up = up_ref[:, head * UNROTATED_WIDTH : (head + 1) * UNROTATED_WIDTH]
        low = (dot(up, plain, ((1,), (1,))) * scale).astype(BF16)
        turned = queries[:, head * step + UNROTATED_WIDTH : (head + 1) * step]
        turned = turn(turned, table_ref[:, :D_ROPE], table_ref[:, D_ROPE:]) * scale
        first = jnp.concatenate([turned, blank], axis=1).astype(BF16)
        second = jnp.concatenate([blank, turned], axis=1).astype(BF16)
        first = dot(unit, first, ((1,), (1,))).astype(BF16)
        second = dot(unit, second, ((1,), (1,))).astype(BF16)
        for c in range(chunks):
            cols = slice(head * span, (head + 1) * span)
            rowsl = slice(c * span, (c + 1) * span)
            qa_ref[c, :lat, cols] = low[:, rowsl]
            qb_ref[c, :lat, cols] = low[:, rowsl]
            qa_ref[c, lat:, cols] = first[:, rowsl]
            qb_ref[c, lat:, cols] = second[:, rowsl]


def attend_body(*refs, groups, chunk, rows):
    qa_ref, qb_ref, mixed_ref = refs[-3:]
    half = rows // 2
    columns = qa_ref.shape[2]
    steps = []
    start = 0
    for size in groups:
        steps += [(refs[start : start + size], 0, qa_ref), (refs[start : start + size], 1, qb_ref)]
        start += size

    def keys_of(step):
        blocks, part, _ = step
        return jnp.concatenate([b[part * half : (part + 1) * half] for b in blocks], axis=0)

    def score_of(step):
        rope = jnp.concatenate([b[rows : rows + half] for b in step[0]], axis=0)
        return dot(jnp.concatenate([keys_of(step), rope], axis=1), step[2][chunk])

    peak = jnp.full((1, columns), MASKED, F32)
    total = jnp.zeros((8, columns), F32)
    weighted = jnp.zeros((LANES, columns), F32)
    coming = score_of(steps[0])
    for i, step in enumerate(steps):
        score = coming
        if i + 1 < len(steps):
            coming = score_of(steps[i + 1])
        top = jnp.maximum(peak, jnp.max(score, axis=0, keepdims=True))
        factor = jnp.exp2(peak - top)
        weight = jnp.exp2(score - top)
        total = total * factor + jnp.sum(weight.reshape(-1, 8, columns), axis=0)
        weighted = weighted * factor + dot(keys_of(step), weight.astype(BF16), ((0,), (0,)))
        peak = top
    mixed_ref[...] = (weighted / jnp.sum(total, axis=0, keepdims=True)).astype(BF16)


def finish_body(
    offset_ref, part_ref, parity_ref, sink_ref, mixed_ref, q_ref, inner_ref, kv_ref, outer_ref, up_ref, ow_ref, ol_ref,
    send_ref, keep_ref, cat_ref, *, chunk, seq_total,
):
    span, columns = send_ref.shape[0], mixed_ref.shape[1]
    mixed = mixed_ref[...]
    heads_l = columns // span
    _, key_heads, lanes, width = q_ref.shape
    group = width // span
    shared = lanes // DH
    own_rows = kv_ref.shape[0]
    even = parity_ref[0] == 0
    pieces = []
    if chunk == 0:
        pieces = [jnp.where(even, outer_ref[...], inner_ref[...])]
    low_row = max(chunk * span - WINDOW, 0)
    high_row = min((chunk + 1) * span + WINDOW, own_rows)
    pieces.append(kv_ref[low_row:high_row])
    if (chunk + 1) * span == own_rows:
        pieces.append(jnp.where(even, inner_ref[...], outer_ref[...]))
    padded = jnp.concatenate(pieces, axis=0)
    offset = offset_ref[0]
    key_pos = lax.broadcasted_iota(jnp.int32, (span + 2 * WINDOW, span), 0) - WINDOW
    query_pos = lax.broadcasted_iota(jnp.int32, (span + 2 * WINDOW, span), 1)
    distance = jnp.abs(key_pos - query_pos)
    spot = key_pos + (offset + chunk * span)
    inside = (distance <= WINDOW) & (spot >= 0) & (spot < seq_total)
    distance = jnp.where(inside, distance.astype(F32), -MASKED)
    distance = jnp.concatenate([distance] * group, axis=1)
    values_at = kv_ref.shape[1] // 2

    def sinks_of(g):
        return jnp.concatenate(
            [sink_ref[g * group + j : g * group + j + 1] for j in range(group)], axis=1
        )

    def slopes_of(g):
        first = part_ref[0] * (key_heads * group) + g * group + 1
        heads = first + lax.broadcasted_iota(jnp.int32, (1, group * span), 1) // span
        return jnp.exp2(heads.astype(F32) * (-8.0 / HEADS_A)) * LOG2E

    def score_of(g):
        at = g // shared * lanes
        return dot(padded[:, at : at + lanes], q_ref[chunk, g])

    coming = score_of(0)
    for g in range(key_heads):
        score = coming
        if g + 1 < key_heads:
            coming = score_of(g + 1)
        at = values_at + g // shared * lanes
        score = score - slopes_of(g) * distance
        sink = sinks_of(g)
        top = jnp.maximum(jnp.max(score, axis=0, keepdims=True), sink)
        weight = jnp.exp2(score - top)
        total = jnp.sum(weight, axis=0, keepdims=True) + jnp.exp2(sink - top)
        out = dot(padded[:, at : at + lanes], weight.astype(BF16), ((0,), (0,)))
        row = g % shared * DH
        out = (out[row : row + DH] / total).astype(BF16)
        for j in range(group):
            head = g * group + j
            cat_ref[head * DH : (head + 1) * DH, :] = out[:, j * span : (j + 1) * span]
    base = key_heads * group * DH
    for head in range(heads_l):
        up = up_ref[:, head * VALUE_WIDTH : (head + 1) * VALUE_WIDTH]
        out = dot(up, mixed[:, head * span : (head + 1) * span], ((0,), (0,)))
        cat_ref[base + head * VALUE_WIDTH : base + (head + 1) * VALUE_WIDTH, :] = out.astype(BF16)
    keep = keep_ref.shape[1]
    win = cat_ref[:base, :]
    low = cat_ref[base:, :]

    def out_of(start):
        return dot(win, ow_ref[:, start : start + keep], ((0,), (0,))) + dot(
            low, ol_ref[:, start : start + keep], ((0,), (0,))
        )

    first = out_of(0)
    second = out_of(keep)
    lower = part_ref[0] == 0
    send_ref[...] = jnp.where(lower, second, first).astype(BF16)
    keep_ref[...] = jnp.where(lower, first, second)


def swap(cells, axis, bit):
    count = lax.axis_size(axis)
    return lax.ppermute(cells, axis, [(i, i ^ bit) for i in range(count)])


def gather(block):
    count = lax.axis_size("sp")
    if count % 4 or count > 16 or count & (count - 1):
        return [[block_of] for block_of in jnp.split(lax.all_gather(block, "sp", axis=0, tiled=True), count)]
    line = [block] + [swap(block, "sp", 4 * k) for k in range(1, count // 4)]
    mine = line + [swap(b, "sp", 2) for b in line]
    return [mine, [swap(b, "sp", 1) for b in mine]]


def per_device(
    activations,
    norm_gain,
    win_query,
    win_key,
    win_value,
    sink_logit,
    lat_query,
    key_value_down_weight,
    rope_key,
    latent_norm_gain,
    key_up_weight,
    value_up_weight,
    out_win,
    out_lat,
):
    rows, half = activations.shape
    features = norm_gain.shape[0]
    part = lax.axis_index("tp").astype(jnp.int32)
    count = lax.axis_size("sp")
    offset = lax.axis_index("sp").astype(jnp.int32) * rows
    shape = jax.ShapeDtypeStruct

    heads = sink_logit.shape[0]
    parity = lax.axis_index("sp").astype(jnp.int32) % 2

    places = (offset + jnp.arange(rows, dtype=jnp.int32)).astype(F32)
    angles = rotary_angles(places, D_ROPE)
    cosines, sines = jnp.cos(angles), jnp.sin(angles)
    table = jnp.concatenate([cosines, cosines, -sines, sines], axis=1)

    lat = key_value_down_weight.shape[1]
    normalized, own, send = call(
        compress_body,
        [shape((rows, half), BF16), shape((rows, lat + LANES), F32), shape((rows, lat + LANES), BF16)],
        [offset[None], part[None], parity[None]], [activations, norm_gain[None], key_value_down_weight, rope_key.T], [],
        2 * rows * half * 192, 8,
        [
            pltpu.VMEM((rows, half), BF16),
            pltpu.VMEM((1, half), F32),
            pltpu.VMEM((half, lat), BF16),
            pltpu.VMEM((rope_key.shape[1], half), BF16),
            pltpu.SemaphoreType.DMA((4,)),
        ],
    )
    got = swap(send, "tp", 1)
    other = swap(normalized, "tp", 1)
    weights = [win_key, win_value, win_query, lat_query]
    partial_sums = call(
        partial(own_body, count=len(weights)),
        [shape((rows, w.shape[1]), F32) for w in weights]
        + [shape((half, w.shape[1]), BF16) for w in weights],
        [part[None]], weights, [normalized],
        2 * rows * half * 1792, 16,
        [pltpu.VMEM((half, w.shape[1]), BF16) for w in weights]
        + [pltpu.SemaphoreType.DMA((2, len(weights)))],
    )
    block, row_scale = call(
        partial(latent_body, features=features),
        [shape((rows + rows // 2, lat), BF16), shape((rows, LANES), F32)],
        [], [], [own, got, table, latent_norm_gain[None]],
        1e6, 4,
    )
    groups = gather(block)

    chunks = rows // WINDOW
    span = rows // chunks
    group = win_query.shape[1] // win_key.shape[1]
    columns = lat_query.shape[1] // (UNROTATED_WIDTH + D_ROPE) * (rows // chunks)
    queries, key_value, inward, outward, table_a, table_b = call(
        project_body,
        [
            shape((chunks, win_key.shape[1] // DH, LANES, group * span), BF16),
            shape((rows, win_key.shape[1] + win_value.shape[1]), BF16),
            shape((WINDOW, win_key.shape[1] + win_value.shape[1]), BF16),
            shape((WINDOW, win_key.shape[1] + win_value.shape[1]), BF16),
            shape((chunks, lat + LANES, columns), BF16),
            shape((chunks, lat + LANES, columns), BF16),
        ],
        [parity[None]], [],
        [other, row_scale, table, *partial_sums, key_up_weight],
        2 * rows * half * 1792, 16,
    )
    inner = lax.ppermute(inward, "sp", [(i, i ^ 1) for i in range(count) if i ^ 1 < count])
    outer = lax.ppermute(
        outward, "sp", [(i, (i - 1 ^ 1) + 1) for i in range(1, count) if (i - 1 ^ 1) + 1 < count]
    )

    sinks = jnp.broadcast_to(sink_logit[:, None] * LOG2E, (heads, LANES))
    kept = []
    flat = [b for group in groups for b in group]
    for c in range(chunks):
        mixed = call(
            partial(attend_body, groups=[len(g) for g in groups], chunk=c, rows=rows),
            shape((lat, columns), BF16), [], [], [*flat, table_a, table_b], 3e9, 32,
        )
        send, keep = call(
            partial(finish_body, chunk=c, seq_total=rows * count),
            [shape((span, half), BF16), shape((span, half), F32)],
            [offset[None], part[None], parity[None]], [],
            [sinks, mixed, queries, inner, key_value, outer, value_up_weight, out_win, out_lat],
            1e9, 16,
            [pltpu.VMEM((out_win.shape[0] + out_lat.shape[0], span), BF16)],
        )
        kept.append((keep, swap(send, "tp", 1)))
    return jnp.concatenate([(keep + got.astype(F32)).astype(BF16) for keep, got in kept], axis=0)


def solution(mesh):
    narrow = mesh.shape["tp"] == 2
    body = per_device if narrow else per_device_wide
    return jax.shard_map(
        body,
        mesh=mesh,
        in_specs=(
            P("sp", "tp"),
            P(),
            P(None, "tp"),
            P(None, "tp"),
            P(None, "tp"),
            P("tp"),
            P(None, "tp"),
            P(),
            P(),
            P(),
            P(None, "tp"),
            P(None, "tp"),
            P("tp", None),
            P("tp", None),
        ),
        out_specs=P("sp", "tp"),
        check_vma=False,
    )
```

```python
from functools import partial

import jax
import jax.numpy as jnp
from jax import lax
from jax.experimental import pallas as pl
from jax.experimental.pallas import tpu as pltpu
from jax.sharding import PartitionSpec as P


HEADS_A = 16
DH = 64
WINDOW = 128
UNROTATED_WIDTH = 128
D_ROPE = 64
VALUE_WIDTH = 128


EPSILON = 1e-06
ROPE_BASE = 10000.0
LOG2E = 1.4426950408889634
LANES = 128
MASKED = -1e30


F32 = jnp.float32
BF16 = jnp.bfloat16


def padded_2(cells, sides, width):
    for axis, dim in sides:
        count = lax.axis_size(axis)
        ends = count - 1
        head = lax.slice_in_dim(cells, 0, width, axis=dim)
        tail = lax.slice_in_dim(cells, cells.shape[dim] - width, cells.shape[dim], axis=dim)
        cells = jnp.concatenate(
            [
                lax.ppermute(tail, axis, [(i, (i + 1) % count) for i in range(ends)]),
                cells,
                lax.ppermute(head, axis, [((i + 1) % count, i) for i in range(ends)]),
            ],
            axis=dim,
        )
    return cells


def rotate(vectors, angles):
    half_width = vectors.shape[-1] // 2
    cosine_table = jnp.cos(angles)
    sine_table = jnp.sin(angles)
    lower_half = vectors[..., :half_width]
    upper_half = vectors[..., half_width:]
    return jnp.concatenate(
        [
            lower_half * cosine_table - upper_half * sine_table,
            lower_half * sine_table + upper_half * cosine_table,
        ],
        axis=-1,
    )


def rotary_angles(places, width):
    frequency = 1.0 / ROPE_BASE ** (jnp.arange(0, width, 2).astype(jnp.float32) / width)
    return places[:, None] * frequency[None, :]


def window_attention(queries, padded, sinks, offset, seq_total, head_start):
    tok_rows = queries.shape[0]
    key_heads = padded.shape[1] // (2 * DH)
    groups = queries.shape[1] // (DH * key_heads)
    key_rows = padded[:, : key_heads * DH].reshape(-1, key_heads, DH)
    value_rows = padded[:, key_heads * DH :].reshape(-1, key_heads, DH)
    grouped = queries.reshape(tok_rows, key_heads, groups, DH)
    scores = jnp.einsum(
        "qhgd,khd->hgqk", grouped, key_rows, preferred_element_type=jnp.float32
    ) * DH ** (-0.5)
    query_pos = offset + jnp.arange(tok_rows, dtype=jnp.int32)
    key_pos = offset - WINDOW + jnp.arange(tok_rows + 2 * WINDOW, dtype=jnp.int32)
    distance = jnp.abs(query_pos[:, None] - key_pos[None, :])
    in_window = (distance <= WINDOW) & (key_pos[None, :] >= 0) & (key_pos[None, :] < seq_total)
    head_ids = head_start + jnp.arange(key_heads * groups, dtype=jnp.int32)
    slopes = jnp.exp2(-8.0 * (head_ids + 1).astype(jnp.float32) / HEADS_A).reshape(
        key_heads, groups
    )
    scores = scores - slopes[:, :, None, None] * distance.astype(jnp.float32)[None, None]
    scores = jnp.where(in_window[None, None], scores, -jnp.inf)
    sink_table = sinks.reshape(key_heads, groups)
    row_peak = jnp.maximum(jnp.max(scores, axis=3), sink_table[:, :, None])
    weights = jnp.exp(scores - row_peak[..., None])
    denominator = jnp.sum(weights, axis=3) + jnp.exp(sink_table[:, :, None] - row_peak)
    blended = jnp.einsum(
        "hgqk,khd->qhgd",
        weights.astype(jnp.bfloat16),
        value_rows,
        preferred_element_type=jnp.float32,
    )
    blended = blended / jnp.transpose(denominator, (2, 0, 1))[..., None]
    return blended.reshape(tok_rows, key_heads * groups * DH).astype(jnp.bfloat16)


def latent_step(running, key_block, query_plain, query_turned):
    row_peak, totals, weighted = running
    keys_plain, values_plain, keys_turned = key_block
    key_count = keys_plain.shape[0]
    head_count = query_plain.shape[1]
    scores = jnp.einsum(
        "qhd,khd->hqk",
        query_plain,
        keys_plain.reshape(key_count, head_count, UNROTATED_WIDTH),
        preferred_element_type=jnp.float32,
    )
    scores = scores + jnp.einsum(
        "qhd,kd->hqk", query_turned, keys_turned, preferred_element_type=jnp.float32
    )
    scores = scores * (UNROTATED_WIDTH + D_ROPE) ** (-0.5)
    new_peak = jnp.maximum(row_peak, jnp.max(scores, axis=2))
    factor = jnp.exp(row_peak - new_peak)
    weights = jnp.exp(scores - new_peak[..., None])
    totals = totals * factor + jnp.sum(weights, axis=2)
    weighted = weighted * factor[..., None] + jnp.einsum(
        "hqk,khd->hqd",
        weights.astype(jnp.bfloat16),
        values_plain.reshape(key_count, head_count, VALUE_WIDTH),
        preferred_element_type=jnp.float32,
    )
    return (new_peak, totals, weighted)


def over_blocks(running, pieces, prepare, attend, block_rows):
    key_count = pieces[0].shape[0]
    stacked = tuple(
        (
            piece_part.reshape((key_count // block_rows, block_rows) + piece_part.shape[1:])
            for piece_part in pieces
        )
    )

    def one_block(state_now, key_block):
        return (attend(state_now, prepare(key_block)), None)

    return lax.scan(one_block, running, stacked)[0]


def per_device_wide(
    activations,
    norm_gain,
    win_query,
    win_key,
    win_value,
    sink_logit,
    lat_query,
    key_value_down_weight,
    rope_key,
    latent_norm_gain,
    key_up_weight,
    value_up_weight,
    out_win,
    out_lat,
):
    tok_rows = activations.shape[0]
    weights_all = (win_query, win_key, win_value, lat_query, key_value_down_weight, rope_key)
    widened = lax.all_gather(activations, "tp", axis=1, tiled=True).astype(jnp.float32)
    normalized = (widened * norm_gain[None, :]).astype(jnp.bfloat16)
    squares = jnp.sum(widened * widened, axis=1)
    totals = tuple(
        (jnp.dot(normalized, weight, preferred_element_type=jnp.float32) for weight in weights_all)
    )
    squares, totals = (squares, totals)
    win_proj, key_proj, value_proj, latq_proj, compressed, rope_proj = totals
    row_scale = lax.rsqrt(squares / norm_gain.shape[0] + EPSILON)[:, None]
    offset = lax.axis_index("sp") * tok_rows
    seq_total = tok_rows * lax.axis_size("sp")
    places = (offset + jnp.arange(tok_rows, dtype=jnp.int32)).astype(jnp.float32)
    angles = rotary_angles(places, D_ROPE)
    win_queries = (win_proj * row_scale).astype(jnp.bfloat16)
    key_value = jnp.concatenate(
        [
            (key_proj * row_scale).astype(jnp.bfloat16),
            (value_proj * row_scale).astype(jnp.bfloat16),
        ],
        axis=1,
    )
    padded = padded_2(key_value, (("sp", 0),), WINDOW)
    head_start = lax.axis_index("tp") * sink_logit.shape[0]
    win_out = window_attention(win_queries, padded, sink_logit, offset, seq_total, head_start)
    head_count = lat_query.shape[1] // (UNROTATED_WIDTH + D_ROPE)
    query_all = (latq_proj * row_scale).reshape(tok_rows, head_count, UNROTATED_WIDTH + D_ROPE)
    query_plain = query_all[..., :UNROTATED_WIDTH].astype(jnp.bfloat16)
    query_turned = rotate(query_all[..., UNROTATED_WIDTH:], angles[:, None, :]).astype(jnp.bfloat16)
    latent = (
        compressed
        * lax.rsqrt(jnp.mean(compressed * compressed, axis=1, keepdims=True) + EPSILON)
        * latent_norm_gain[None, :]
    ).astype(jnp.bfloat16)
    key_rotary = rotate(rope_proj * row_scale, angles).astype(jnp.bfloat16)
    attend = partial(latent_step, query_plain=query_plain, query_turned=query_turned)

    def expand(key_block):
        return (
            jnp.dot(key_block[0], key_up_weight, preferred_element_type=jnp.float32).astype(
                jnp.bfloat16
            ),
            jnp.dot(key_block[0], value_up_weight, preferred_element_type=jnp.float32).astype(
                jnp.bfloat16
            ),
            key_block[1],
        )

    _, totals_lat, weighted = over_blocks(
        (
            jnp.full((head_count, tok_rows), -jnp.inf, jnp.float32),
            jnp.zeros((head_count, tok_rows), jnp.float32),
            jnp.zeros((head_count, tok_rows, VALUE_WIDTH), jnp.float32),
        ),
        (
            lax.all_gather(latent, "sp", axis=0, tiled=True),
            lax.all_gather(key_rotary, "sp", axis=0, tiled=True),
        ),
        expand,
        attend,
        2048,
    )
    lat_out = (
        (weighted / totals_lat[..., None])
        .transpose(1, 0, 2)
        .reshape(tok_rows, head_count * VALUE_WIDTH)
    )
    lat_out = lat_out.astype(jnp.bfloat16)
    terms = jnp.dot(win_out, out_win, preferred_element_type=jnp.float32) + jnp.dot(
        lat_out, out_lat, preferred_element_type=jnp.float32
    )
    return lax.psum_scatter(terms.astype(jnp.bfloat16), "tp", scatter_dimension=1, tiled=True)


def dot(a, b, dims=((1,), (0,))):
    return lax.dot_general(a, b, (dims, ((), ())), preferred_element_type=F32)


def whole(count):
    return [pl.BlockSpec(memory_space=pltpu.VMEM)] * count


def scalars(count):
    return [pl.BlockSpec(memory_space=pltpu.SMEM)] * count


def call(body, shapes, smem, hbm, operands, flops, mib, scratch=()):
    single = not isinstance(shapes, (list, tuple))
    outs = [shapes] if single else list(shapes)
    result = pl.pallas_call(
        body,
        out_shape=outs,
        in_specs=scalars(len(smem))
        + [pl.BlockSpec(memory_space=pltpu.HBM)] * len(hbm)
        + whole(len(operands)),
        out_specs=whole(len(outs)),
        scratch_shapes=list(scratch),
        cost_estimate=pl.CostEstimate(
            flops=int(flops),
            bytes_accessed=sum(x.size * x.dtype.itemsize for x in [*hbm, *operands]),
            transcendentals=0,
        ),
        compiler_params=pltpu.CompilerParams(vmem_limit_bytes=mib * 2**20),
    )(*smem, *[pltpu.with_memory_space_constraint(x, pltpu.HBM) for x in hbm], *operands)
    return result[0] if single else result


def compress_body(
    offset_ref, part_ref, parity_ref, other_ref, x_hbm, gain_hbm, down_hbm, rope_hbm, norm_ref, own_ref, send_ref,
    x_ref, gain_ref, down_ref, rope_ref, sems,
):
    rows, half = x_hbm.shape
    del offset_ref, parity_ref, other_ref
    start = pl.multiple_of(part_ref[0] * half, half)
    copies = [
        pltpu.make_async_copy(x_hbm, x_ref, sems.at[0]),
        pltpu.make_async_copy(gain_hbm.at[:, pl.ds(start, half)], gain_ref, sems.at[3]),
        pltpu.make_async_copy(down_hbm.at[pl.ds(start, half), :], down_ref, sems.at[1]),
        pltpu.make_async_copy(rope_hbm.at[:, pl.ds(start, half)], rope_ref, sems.at[2]),
    ]
    for copy in copies:
        copy.start()
    copies[0].wait()
    copies[1].wait()
    wide = x_ref[...].astype(F32)
    normalized = (wide * gain_ref[...]).astype(BF16)
    norm_ref[...] = normalized
    squares = jnp.sum(wide * wide, axis=1, keepdims=True)
    copies[2].wait()
    compressed = dot(normalized, down_ref[...])
    copies[3].wait()
    rope = dot(normalized, rope_ref[...], ((1,), (1,)))
    high = squares.astype(BF16).astype(F32)
    lane = lax.broadcasted_iota(jnp.int32, (rows, LANES), 1)
    rope = jnp.concatenate([rope, jnp.zeros((rows, LANES - rope.shape[1]), F32)], axis=1)
    width = compressed.shape[1]
    own_ref[:, :width] = compressed
    own_ref[:, width:] = jnp.where(lane == LANES - 1, squares, jnp.where(lane == LANES - 2, 0.0, rope))
    send_ref[:, :width] = compressed.astype(BF16)
    send_ref[:, width:] = jnp.where(
        lane == LANES - 1, high, jnp.where(lane == LANES - 2, squares - high, rope)
    ).astype(BF16)


def turn(vectors, cosines, sines):
    half = vectors.shape[1] // 2
    swapped = jnp.concatenate([vectors[:, half:], vectors[:, :half]], axis=1)
    return vectors * cosines + swapped * sines


def latent_body(own_ref, got_ref, table_ref, gain_ref, block_ref, scale_ref, *, features):
    rows = own_ref.shape[0]
    total = own_ref[...] + got_ref[...].astype(F32)
    width = gain_ref.shape[1]
    compressed = total[:, :width]
    rest = total[:, width:]
    squares = rest[:, LANES - 1 :] + rest[:, LANES - 2 : LANES - 1]
    row_scale = lax.rsqrt(squares / features + EPSILON)
    scale_ref[...] = jnp.broadcast_to(row_scale, scale_ref.shape)
    mean = jnp.mean(compressed * compressed, axis=1, keepdims=True)
    block_ref[:rows] = (compressed * lax.rsqrt(mean + EPSILON) * gain_ref[...]).astype(BF16)
    rope = turn(rest[:, :D_ROPE] * row_scale, table_ref[:, :D_ROPE], table_ref[:, D_ROPE:])
    packed = jnp.concatenate([rope[: rows // 2], rope[rows // 2 :]], axis=1)
    block_ref[rows:] = packed.astype(BF16)


def own_body(part_ref, *refs, count):
    weights = refs[:count]
    own_ref = refs[count]
    sums = refs[count + 1 : 2 * count + 1]
    rests = refs[2 * count + 1 : 3 * count + 1]
    mines = refs[3 * count + 1 : 4 * count + 1]
    sems = refs[-1]
    half = own_ref.shape[1]
    part = part_ref[0]
    mine = pl.multiple_of(part * half, half)
    theirs = pl.multiple_of((1 - part) * half, half)
    first = [
        pltpu.make_async_copy(w.at[pl.ds(mine, half), :], m, sems.at[0, i])
        for i, (w, m) in enumerate(zip(weights, mines))
    ]
    second = [
        pltpu.make_async_copy(w.at[pl.ds(theirs, half), :], r, sems.at[1, i])
        for i, (w, r) in enumerate(zip(weights, rests))
    ]
    for copy in first + second:
        copy.start()
    own = own_ref[...]
    for copy, mine_ref, sum_ref in zip(first, mines, sums):
        copy.wait()
        sum_ref[...] = dot(own, mine_ref[...])
    for copy in second:
        copy.wait()


def project_body(
    parity_ref, got_ref, scale_ref, table_ref, sk_ref, sv_ref, sq_ref, sl_ref, wk_ref, wv_ref, wq_ref, wl_ref,
    up_ref, q_ref, kv_ref, in_ref, out_ref, qa_ref, qb_ref,
):
    got = got_ref[...]
    rows = got.shape[0]
    row_scale = scale_ref[:, :1]

    def project(sum_ref, w_ref):
        return (sum_ref[...] + dot(got, w_ref[...])) * row_scale

    width = wk_ref.shape[1]
    kv_ref[:, :width] = project(sk_ref, wk_ref).astype(BF16)
    kv_ref[:, width:] = project(sv_ref, wv_ref).astype(BF16)
    even = parity_ref[0] == 0
    head = kv_ref[:WINDOW]
    tail = kv_ref[rows - WINDOW :]
    in_ref[...] = jnp.where(even, tail, head)
    out_ref[...] = jnp.where(even, head, tail)
    win = (project(sq_ref, wq_ref) * (DH**-0.5 * LOG2E)).astype(BF16)
    queries = project(sl_ref, wl_ref)
    step = UNROTATED_WIDTH + D_ROPE
    scale = step**-0.5 * LOG2E
    row = lax.broadcasted_iota(jnp.int32, (LANES, LANES), 0)
    col = lax.broadcasted_iota(jnp.int32, (LANES, LANES), 1)
    unit = jnp.where(row == col, 1.0, 0.0).astype(BF16)
    blank = jnp.zeros((rows, LANES - D_ROPE), F32)
    chunks = qa_ref.shape[0]
    span = rows // chunks
    shared = LANES // DH
    group = win.shape[1] // width
    for g in range(width // DH):
        pair = dot(unit, win[:, g * group * DH : (g + 1) * group * DH], ((1,), (1,))).astype(BF16)
        spot = g % shared * DH
        for c in range(chunks):
            q_ref[c, g] = jnp.zeros(q_ref.shape[2:], BF16)
            for j in range(group):
                q_ref[c, g, spot : spot + DH, j * span : (j + 1) * span] = pair[
                    j * DH : (j + 1) * DH, c * span : (c + 1) * span
                ]
    lat = up_ref.shape[0]
    for head in range(wl_ref.shape[1] // step):
        plain = queries[:, head * step : head * step + UNROTATED_WIDTH].astype(BF16)
        up = up_ref[:, head * UNROTATED_WIDTH : (head + 1) * UNROTATED_WIDTH]
        low = (dot(up, plain, ((1,), (1,))) * scale).astype(BF16)
        turned = queries[:, head * step + UNROTATED_WIDTH : (head + 1) * step]
        turned = turn(turned, table_ref[:, :D_ROPE], table_ref[:, D_ROPE:]) * scale
        first = jnp.concatenate([turned, blank], axis=1).astype(BF16)
        second = jnp.concatenate([blank, turned], axis=1).astype(BF16)
        first = dot(unit, first, ((1,), (1,))).astype(BF16)
        second = dot(unit, second, ((1,), (1,))).astype(BF16)
        for c in range(chunks):
            cols = slice(head * span, (head + 1) * span)
            rowsl = slice(c * span, (c + 1) * span)
            qa_ref[c, :lat, cols] = low[:, rowsl]
            qb_ref[c, :lat, cols] = low[:, rowsl]
            qa_ref[c, lat:, cols] = first[:, rowsl]
            qb_ref[c, lat:, cols] = second[:, rowsl]


def attend(groups, qa, qb, state):
    rows = groups[0][0].shape[0] * 2 // 3
    half = rows // 2
    columns = qa.shape[1]
    steps = [(blocks, part, table) for blocks in groups for part, table in ((0, qa), (1, qb))]

    def keys_of(step):
        blocks, part, _ = step
        return jnp.concatenate([b[part * half : (part + 1) * half] for b in blocks], axis=0)

    def score_of(step):
        rope = jnp.concatenate([b[rows : rows + half] for b in step[0]], axis=0)
        return dot(jnp.concatenate([keys_of(step), rope], axis=1), step[2])

    peak, total, weighted = state
    coming = score_of(steps[0])
    for i, step in enumerate(steps):
        score = coming
        if i + 1 < len(steps):
            coming = score_of(steps[i + 1])
        top = jnp.max(score, axis=0, keepdims=True)
        if peak is not None:
            top = jnp.maximum(peak, top)
        weight = jnp.exp2(score - top)
        new_total = jnp.sum(weight.reshape(-1, 8, columns), axis=0)
        new_weighted = dot(keys_of(step), weight.astype(BF16), ((0,), (0,)))
        if peak is not None:
            factor = jnp.exp2(peak - top)
            new_total = total * factor + new_total
            new_weighted = weighted * factor + new_weighted
        peak, total, weighted = top, new_total, new_weighted
    return peak, total, weighted


def begin_body(chunk_ref, *refs, groups):
    chunk = chunk_ref[0]
    qa_ref, qb_ref, stat_ref, sum_ref = refs[sum(groups) :]
    blocks = list(refs[: sum(groups)])
    parts = [[blocks.pop(0) for _ in range(size)] for size in groups]
    peak, total, weighted = attend(parts, qa_ref[chunk], qb_ref[chunk], (None, None, None))
    stat_ref[:8] = jnp.broadcast_to(peak, total.shape)
    stat_ref[8:] = total
    sum_ref[...] = weighted


def finish_body(
    offset_ref, part_ref, chunk_ref, *refs, groups, seq_total,
):
    count = sum(groups)
    (
        qa_ref, qb_ref, stat_ref, sum_ref, sink_ref, q_ref, halo_ref, kv_ref, up_ref,
        ow_ref, ol_ref, send_ref, keep_ref, cat_ref, pad_ref,
    ) = refs[count:]
    chunk = chunk_ref[0]
    total, weighted = stat_ref[8:], sum_ref[...]
    if count:
        blocks = list(refs[:count])
        parts = [[blocks.pop(0) for _ in range(size)] for size in groups]
        state = (stat_ref[:1], total, weighted)
        _, total, weighted = attend(parts, qa_ref[chunk], qb_ref[chunk], state)
    mixed = (weighted / jnp.sum(total, axis=0, keepdims=True)).astype(BF16)
    span, columns = send_ref.shape[0], mixed.shape[1]
    heads_l = columns // span
    _, key_heads, lanes, width = q_ref.shape
    group = width // span
    shared = lanes // DH
    own_rows = kv_ref.shape[0]
    pad_ref[pl.ds(pl.multiple_of((1 - chunk) * WINDOW, WINDOW), own_rows), :] = kv_ref[...]
    pad_ref[pl.ds(pl.multiple_of(chunk * own_rows, WINDOW), WINDOW), :] = halo_ref[...]
    padded = pad_ref[...]
    offset = offset_ref[0]
    key_pos = lax.broadcasted_iota(jnp.int32, (span + 2 * WINDOW, span), 0) - WINDOW
    query_pos = lax.broadcasted_iota(jnp.int32, (span + 2 * WINDOW, span), 1)
    distance = jnp.abs(key_pos - query_pos)
    spot = key_pos + (offset + chunk * span)
    inside = (distance <= WINDOW) & (spot >= 0) & (spot < seq_total)
    distance = jnp.where(inside, distance.astype(F32), -MASKED)
    distance = jnp.concatenate([distance] * group, axis=1)
    values_at = kv_ref.shape[1] // 2

    def sinks_of(g):
        return jnp.concatenate(
            [sink_ref[g * group + j : g * group + j + 1] for j in range(group)], axis=1
        )

    def slopes_of(g):
        first = part_ref[0] * (key_heads * group) + g * group + 1
        heads = first + lax.broadcasted_iota(jnp.int32, (1, group * span), 1) // span
        return jnp.exp2(heads.astype(F32) * (-8.0 / HEADS_A)) * LOG2E

    def score_of(g):
        at = g // shared * lanes
        return dot(padded[:, at : at + lanes], q_ref[chunk, g])

    coming = score_of(0)
    for g in range(key_heads):
        score = coming
        if g + 1 < key_heads:
            coming = score_of(g + 1)
        at = values_at + g // shared * lanes
        score = score - slopes_of(g) * distance
        sink = sinks_of(g)
        top = jnp.maximum(jnp.max(score, axis=0, keepdims=True), sink)
        weight = jnp.exp2(score - top)
        total = jnp.sum(weight, axis=0, keepdims=True) + jnp.exp2(sink - top)
        out = dot(padded[:, at : at + lanes], weight.astype(BF16), ((0,), (0,)))
        row = g % shared * DH
        out = (out[row : row + DH] / total).astype(BF16)
        for j in range(group):
            head = g * group + j
            cat_ref[head * DH : (head + 1) * DH, :] = out[:, j * span : (j + 1) * span]
    base = key_heads * group * DH
    for head in range(heads_l):
        up = up_ref[:, head * VALUE_WIDTH : (head + 1) * VALUE_WIDTH]
        out = dot(up, mixed[:, head * span : (head + 1) * span], ((0,), (0,)))
        cat_ref[base + head * VALUE_WIDTH : base + (head + 1) * VALUE_WIDTH, :] = out.astype(BF16)
    keep = keep_ref.shape[1]
    win = cat_ref[:base, :]
    low = cat_ref[base:, :]

    def out_of(start):
        return dot(win, ow_ref[:, start : start + keep], ((0,), (0,))) + dot(
            low, ol_ref[:, start : start + keep], ((0,), (0,))
        )

    first = out_of(0)
    second = out_of(keep)
    lower = part_ref[0] == 0
    send_ref[...] = jnp.where(lower, second, first).astype(BF16)
    keep_ref[...] = jnp.where(lower, first, second)


def store_body(chunk_ref, *refs, fresh):
    keep_ref, got_ref, out_ref, row_ref, sem = refs if fresh else refs[1:]
    span = keep_ref.shape[0]
    row_ref[...] = (keep_ref[...] + got_ref[...].astype(F32)).astype(BF16)
    place = pl.multiple_of(chunk_ref[0] * span, span)
    copy = pltpu.make_async_copy(row_ref, out_ref.at[pl.ds(place, span), :], sem)
    copy.start()
    copy.wait()


def store(chunk, keep, got, rows, whole_out=None):
    fresh = whole_out is None
    hbm = pl.BlockSpec(memory_space=pltpu.HBM)
    return pl.pallas_call(
        partial(store_body, fresh=fresh),
        out_shape=jax.ShapeDtypeStruct((rows, keep.shape[1]), BF16),
        in_specs=scalars(1) + ([] if fresh else [hbm]) + whole(2),
        out_specs=hbm,
        scratch_shapes=[pltpu.VMEM(keep.shape, BF16), pltpu.SemaphoreType.DMA],
        input_output_aliases={} if fresh else {1: 0},
        name="store" if fresh else "store_rest",
        compiler_params=pltpu.CompilerParams(vmem_limit_bytes=4 * 2**20),
    )(chunk[None], *([] if fresh else [whole_out]), keep, got)


def swap(cells, axis, bit):
    count = lax.axis_size(axis)
    return lax.ppermute(cells, axis, [(i, i ^ bit) for i in range(count)])


def gather(block):
    count = lax.axis_size("sp")
    if count % 4 or count > 16 or count & (count - 1):
        pieces = jnp.split(lax.all_gather(block, "sp", axis=0, tiled=True), count)
        return [pieces[: count // 2], pieces[count // 2 :]]
    line = [block] + [swap(block, "sp", 4 * k) for k in range(1, count // 4)]
    mine = line + [swap(b, "sp", 2) for b in line]
    across = [swap(b, "sp", 1) for b in mine]
    late = len(line) // 2
    early = len(mine) - late
    return [
        [*mine[:late], *across[:late], *mine[late:early], *across[late:early]],
        [*mine[early:], *across[early:]],
    ]


def per_device(
    activations,
    norm_gain,
    win_query,
    win_key,
    win_value,
    sink_logit,
    lat_query,
    key_value_down_weight,
    rope_key,
    latent_norm_gain,
    key_up_weight,
    value_up_weight,
    out_win,
    out_lat,
):
    rows, half = activations.shape
    features = norm_gain.shape[0]
    part = lax.axis_index("tp").astype(jnp.int32)
    count = lax.axis_size("sp")
    offset = lax.axis_index("sp").astype(jnp.int32) * rows
    shape = jax.ShapeDtypeStruct

    heads = sink_logit.shape[0]
    parity = lax.axis_index("sp").astype(jnp.int32) % 2
    flip = 1 - parity

    places = (offset + jnp.arange(rows, dtype=jnp.int32)).astype(F32)
    angles = rotary_angles(places, D_ROPE)
    cosines, sines = jnp.cos(angles), jnp.sin(angles)
    table = jnp.concatenate([cosines, cosines, -sines, sines], axis=1)

    lat = key_value_down_weight.shape[1]
    normalized, own, send = call(
        compress_body,
        [shape((rows, half), BF16), shape((rows, lat + LANES), F32), shape((rows, lat + LANES), BF16)],
        [offset[None], part[None], parity[None], flip[None]], [activations, norm_gain[None], key_value_down_weight, rope_key.T], [],
        2 * rows * half * 192, 8,
        [
            pltpu.VMEM((rows, half), BF16),
            pltpu.VMEM((1, half), F32),
            pltpu.VMEM((half, lat), BF16),
            pltpu.VMEM((rope_key.shape[1], half), BF16),
            pltpu.SemaphoreType.DMA((4,)),
        ],
    )
    got = swap(send, "tp", 1)
    other = swap(normalized, "tp", 1)
    weights = [win_key, win_value, win_query, lat_query]
    partial_sums = call(
        partial(own_body, count=len(weights)),
        [shape((rows, w.shape[1]), F32) for w in weights]
        + [shape((half, w.shape[1]), BF16) for w in weights],
        [part[None]], weights, [normalized],
        2 * rows * half * 1792, 16,
        [pltpu.VMEM((half, w.shape[1]), BF16) for w in weights]
        + [pltpu.SemaphoreType.DMA((2, len(weights)))],
    )
    block, row_scale = call(
        partial(latent_body, features=features),
        [shape((rows + rows // 2, lat), BF16), shape((rows, LANES), F32)],
        [], [], [own, got, table, latent_norm_gain[None]],
        1e6, 4,
    )
    groups = gather(block)

    chunks = rows // WINDOW
    span = rows // chunks
    group = win_query.shape[1] // win_key.shape[1]
    columns = lat_query.shape[1] // (UNROTATED_WIDTH + D_ROPE) * (rows // chunks)
    queries, key_value, inward, outward, table_a, table_b = call(
        project_body,
        [
            shape((chunks, win_key.shape[1] // DH, LANES, group * span), BF16),
            shape((rows, win_key.shape[1] + win_value.shape[1]), BF16),
            shape((WINDOW, win_key.shape[1] + win_value.shape[1]), BF16),
            shape((WINDOW, win_key.shape[1] + win_value.shape[1]), BF16),
            shape((chunks, lat + LANES, columns), BF16),
            shape((chunks, lat + LANES, columns), BF16),
        ],
        [parity[None]], [],
        [other, row_scale, table, *partial_sums, key_up_weight],
        2 * rows * half * 1792, 16,
    )
    inner = lax.ppermute(inward, "sp", [(i, i ^ 1) for i in range(count) if i ^ 1 < count])

    def partner(i):
        other = i + 1 if i % 2 else i - 1
        return other if 0 <= other < count else i

    outer = lax.ppermute(
        outward, "sp", [(i, partner(i)) for i in range(count)]
    )

    sinks = jnp.broadcast_to(sink_logit[:, None] * LOG2E, (heads, LANES))
    kept = []
    assert chunks == 2
    result = None
    order = (flip, parity)
    for c, (chunk, halo) in enumerate(zip(order, (inner, outer))):
        first = groups[:1] if c == 0 else groups
        last = groups[1:] if c == 0 else []
        sizes = []
        for g in first:
            sizes += [len(g) // 2, len(g) - len(g) // 2] if len(g) > 8 else [len(g)]
        state = call(
            partial(begin_body, groups=sizes),
            [shape((16, columns), F32), shape((lat, columns), F32)],
            [chunk[None]], [], [*(b for g in first for b in g), table_a, table_b], 3e9, 32,
        )
        send, keep = call(
            partial(finish_body, groups=[len(g) for g in last], seq_total=rows * count),
            [shape((span, half), BF16), shape((span, half), F32)],
            [offset[None], part[None], chunk[None]], [],
            [
                *(b for g in last for b in g), table_a, table_b, *state, sinks, queries, halo,
                key_value, value_up_weight, out_win, out_lat,
            ],
            1e9, 16,
            [
                pltpu.VMEM((out_win.shape[0] + out_lat.shape[0], span), BF16),
                pltpu.VMEM((rows + WINDOW, key_value.shape[1]), BF16),
            ],
        )
        kept.append((chunk, keep, swap(send, "tp", 1)))
    for chunk, keep, got in kept:
        result = store(chunk, keep, got, rows, result)
    return result


def solution(mesh):
    narrow = mesh.shape["tp"] == 2
    body = per_device if narrow else per_device_wide
    return jax.shard_map(
        body,
        mesh=mesh,
        in_specs=(
            P("sp", "tp"),
            P(),
            P(None, "tp"),
            P(None, "tp"),
            P(None, "tp"),
            P("tp"),
            P(None, "tp"),
            P(),
            P(),
            P(),
            P(None, "tp"),
            P(None, "tp"),
            P("tp", None),
            P("tp", None),
        ),
        out_specs=P("sp", "tp"),
        check_vma=False,
    )
```

```python
from functools import partial

import jax
import jax.numpy as jnp
import numpy as np
from jax import lax
from jax.experimental import pallas as pl
from jax.experimental.pallas import tpu as pltpu
from jax.sharding import PartitionSpec as P


HEADS_A = 16
DH = 64
WINDOW = 128
UNROTATED_WIDTH = 128
D_ROPE = 64
VALUE_WIDTH = 128


EPSILON = 1e-06
ROPE_BASE = 10000.0
LOG2E = 1.4426950408889634
LANES = 128
MASKED = -1e30


F32 = jnp.float32
BF16 = jnp.bfloat16


def padded_2(cells, sides, width):
    for axis, dim in sides:
        count = lax.axis_size(axis)
        ends = count - 1
        head = lax.slice_in_dim(cells, 0, width, axis=dim)
        tail = lax.slice_in_dim(cells, cells.shape[dim] - width, cells.shape[dim], axis=dim)
        cells = jnp.concatenate(
            [
                lax.ppermute(tail, axis, [(i, (i + 1) % count) for i in range(ends)]),
                cells,
                lax.ppermute(head, axis, [((i + 1) % count, i) for i in range(ends)]),
            ],
            axis=dim,
        )
    return cells


def rotate(vectors, angles):
    half_width = vectors.shape[-1] // 2
    cosine_table = jnp.cos(angles)
    sine_table = jnp.sin(angles)
    lower_half = vectors[..., :half_width]
    upper_half = vectors[..., half_width:]
    return jnp.concatenate(
        [
            lower_half * cosine_table - upper_half * sine_table,
            lower_half * sine_table + upper_half * cosine_table,
        ],
        axis=-1,
    )


def rotary_angles(places, width):
    frequency = 1.0 / ROPE_BASE ** (jnp.arange(0, width, 2).astype(jnp.float32) / width)
    return places[:, None] * frequency[None, :]


def window_attention(queries, padded, sinks, offset, seq_total, head_start):
    tok_rows = queries.shape[0]
    key_heads = padded.shape[1] // (2 * DH)
    groups = queries.shape[1] // (DH * key_heads)
    key_rows = padded[:, : key_heads * DH].reshape(-1, key_heads, DH)
    value_rows = padded[:, key_heads * DH :].reshape(-1, key_heads, DH)
    grouped = queries.reshape(tok_rows, key_heads, groups, DH)
    scores = jnp.einsum(
        "qhgd,khd->hgqk", grouped, key_rows, preferred_element_type=jnp.float32
    ) * DH ** (-0.5)
    query_pos = offset + jnp.arange(tok_rows, dtype=jnp.int32)
    key_pos = offset - WINDOW + jnp.arange(tok_rows + 2 * WINDOW, dtype=jnp.int32)
    distance = jnp.abs(query_pos[:, None] - key_pos[None, :])
    in_window = (distance <= WINDOW) & (key_pos[None, :] >= 0) & (key_pos[None, :] < seq_total)
    head_ids = head_start + jnp.arange(key_heads * groups, dtype=jnp.int32)
    slopes = jnp.exp2(-8.0 * (head_ids + 1).astype(jnp.float32) / HEADS_A).reshape(
        key_heads, groups
    )
    scores = scores - slopes[:, :, None, None] * distance.astype(jnp.float32)[None, None]
    scores = jnp.where(in_window[None, None], scores, -jnp.inf)
    sink_table = sinks.reshape(key_heads, groups)
    row_peak = jnp.maximum(jnp.max(scores, axis=3), sink_table[:, :, None])
    weights = jnp.exp(scores - row_peak[..., None])
    denominator = jnp.sum(weights, axis=3) + jnp.exp(sink_table[:, :, None] - row_peak)
    blended = jnp.einsum(
        "hgqk,khd->qhgd",
        weights.astype(jnp.bfloat16),
        value_rows,
        preferred_element_type=jnp.float32,
    )
    blended = blended / jnp.transpose(denominator, (2, 0, 1))[..., None]
    return blended.reshape(tok_rows, key_heads * groups * DH).astype(jnp.bfloat16)


def latent_step(running, key_block, query_plain, query_turned):
    row_peak, totals, weighted = running
    keys_plain, values_plain, keys_turned = key_block
    key_count = keys_plain.shape[0]
    head_count = query_plain.shape[1]
    scores = jnp.einsum(
        "qhd,khd->hqk",
        query_plain,
        keys_plain.reshape(key_count, head_count, UNROTATED_WIDTH),
        preferred_element_type=jnp.float32,
    )
    scores = scores + jnp.einsum(
        "qhd,kd->hqk", query_turned, keys_turned, preferred_element_type=jnp.float32
    )
    scores = scores * (UNROTATED_WIDTH + D_ROPE) ** (-0.5)
    new_peak = jnp.maximum(row_peak, jnp.max(scores, axis=2))
    factor = jnp.exp(row_peak - new_peak)
    weights = jnp.exp(scores - new_peak[..., None])
    totals = totals * factor + jnp.sum(weights, axis=2)
    weighted = weighted * factor[..., None] + jnp.einsum(
        "hqk,khd->hqd",
        weights.astype(jnp.bfloat16),
        values_plain.reshape(key_count, head_count, VALUE_WIDTH),
        preferred_element_type=jnp.float32,
    )
    return (new_peak, totals, weighted)


def over_blocks(running, pieces, prepare, attend, block_rows):
    key_count = pieces[0].shape[0]
    stacked = tuple(
        (
            piece_part.reshape((key_count // block_rows, block_rows) + piece_part.shape[1:])
            for piece_part in pieces
        )
    )

    def one_block(state_now, key_block):
        return (attend(state_now, prepare(key_block)), None)

    return lax.scan(one_block, running, stacked)[0]


def per_device_wide(
    activations,
    norm_gain,
    win_query,
    win_key,
    win_value,
    sink_logit,
    lat_query,
    key_value_down_weight,
    rope_key,
    latent_norm_gain,
    key_up_weight,
    value_up_weight,
    out_win,
    out_lat,
):
    tok_rows = activations.shape[0]
    weights_all = (win_query, win_key, win_value, lat_query, key_value_down_weight, rope_key)
    widened = lax.all_gather(activations, "tp", axis=1, tiled=True).astype(jnp.float32)
    normalized = (widened * norm_gain[None, :]).astype(jnp.bfloat16)
    squares = jnp.sum(widened * widened, axis=1)
    totals = tuple(
        (jnp.dot(normalized, weight, preferred_element_type=jnp.float32) for weight in weights_all)
    )
    squares, totals = (squares, totals)
    win_proj, key_proj, value_proj, latq_proj, compressed, rope_proj = totals
    row_scale = lax.rsqrt(squares / norm_gain.shape[0] + EPSILON)[:, None]
    offset = lax.axis_index("sp") * tok_rows
    seq_total = tok_rows * lax.axis_size("sp")
    places = (offset + jnp.arange(tok_rows, dtype=jnp.int32)).astype(jnp.float32)
    angles = rotary_angles(places, D_ROPE)
    win_queries = (win_proj * row_scale).astype(jnp.bfloat16)
    key_value = jnp.concatenate(
        [
            (key_proj * row_scale).astype(jnp.bfloat16),
            (value_proj * row_scale).astype(jnp.bfloat16),
        ],
        axis=1,
    )
    padded = padded_2(key_value, (("sp", 0),), WINDOW)
    head_start = lax.axis_index("tp") * sink_logit.shape[0]
    win_out = window_attention(win_queries, padded, sink_logit, offset, seq_total, head_start)
    head_count = lat_query.shape[1] // (UNROTATED_WIDTH + D_ROPE)
    query_all = (latq_proj * row_scale).reshape(tok_rows, head_count, UNROTATED_WIDTH + D_ROPE)
    query_plain = query_all[..., :UNROTATED_WIDTH].astype(jnp.bfloat16)
    query_turned = rotate(query_all[..., UNROTATED_WIDTH:], angles[:, None, :]).astype(jnp.bfloat16)
    latent = (
        compressed
        * lax.rsqrt(jnp.mean(compressed * compressed, axis=1, keepdims=True) + EPSILON)
        * latent_norm_gain[None, :]
    ).astype(jnp.bfloat16)
    key_rotary = rotate(rope_proj * row_scale, angles).astype(jnp.bfloat16)
    attend = partial(latent_step, query_plain=query_plain, query_turned=query_turned)

    def expand(key_block):
        return (
            jnp.dot(key_block[0], key_up_weight, preferred_element_type=jnp.float32).astype(
                jnp.bfloat16
            ),
            jnp.dot(key_block[0], value_up_weight, preferred_element_type=jnp.float32).astype(
                jnp.bfloat16
            ),
            key_block[1],
        )

    _, totals_lat, weighted = over_blocks(
        (
            jnp.full((head_count, tok_rows), -jnp.inf, jnp.float32),
            jnp.zeros((head_count, tok_rows), jnp.float32),
            jnp.zeros((head_count, tok_rows, VALUE_WIDTH), jnp.float32),
        ),
        (
            lax.all_gather(latent, "sp", axis=0, tiled=True),
            lax.all_gather(key_rotary, "sp", axis=0, tiled=True),
        ),
        expand,
        attend,
        2048,
    )
    lat_out = (
        (weighted / totals_lat[..., None])
        .transpose(1, 0, 2)
        .reshape(tok_rows, head_count * VALUE_WIDTH)
    )
    lat_out = lat_out.astype(jnp.bfloat16)
    terms = jnp.dot(win_out, out_win, preferred_element_type=jnp.float32) + jnp.dot(
        lat_out, out_lat, preferred_element_type=jnp.float32
    )
    return lax.psum_scatter(terms.astype(jnp.bfloat16), "tp", scatter_dimension=1, tiled=True)


def dot(a, b, dims=((1,), (0,))):
    return lax.dot_general(a, b, (dims, ((), ())), preferred_element_type=F32)


def whole(count):
    return [pl.BlockSpec(memory_space=pltpu.VMEM)] * count


def scalars(count):
    return [pl.BlockSpec(memory_space=pltpu.SMEM)] * count


def call(body, shapes, smem, hbm, operands, flops, mib, scratch=()):
    single = not isinstance(shapes, (list, tuple))
    outs = [shapes] if single else list(shapes)
    result = pl.pallas_call(
        body,
        out_shape=outs,
        in_specs=scalars(len(smem))
        + [pl.BlockSpec(memory_space=pltpu.HBM)] * len(hbm)
        + whole(len(operands)),
        out_specs=whole(len(outs)),
        scratch_shapes=list(scratch),
        cost_estimate=pl.CostEstimate(
            flops=int(flops),
            bytes_accessed=sum(x.size * x.dtype.itemsize for x in [*hbm, *operands]),
            transcendentals=0,
        ),
        compiler_params=pltpu.CompilerParams(vmem_limit_bytes=mib * 2**20),
    )(*smem, *[pltpu.with_memory_space_constraint(x, pltpu.HBM) for x in hbm], *operands)
    return result[0] if single else result


def compress_body(
    offset_ref, part_ref, parity_ref, other_ref, x_hbm, gain_hbm, down_hbm, rope_hbm, norm_ref, own_ref, send_ref,
    x_ref, gain_ref, down_ref, rope_ref, sems,
):
    rows, half = x_hbm.shape
    del offset_ref, parity_ref, other_ref
    start = pl.multiple_of(part_ref[0] * half, half)
    copies = [
        pltpu.make_async_copy(x_hbm, x_ref, sems.at[0]),
        pltpu.make_async_copy(gain_hbm.at[:, pl.ds(start, half)], gain_ref, sems.at[3]),
        pltpu.make_async_copy(down_hbm.at[pl.ds(start, half), :], down_ref, sems.at[1]),
        pltpu.make_async_copy(rope_hbm.at[:, pl.ds(start, half)], rope_ref, sems.at[2]),
    ]
    for copy in copies:
        copy.start()
    copies[0].wait()
    copies[1].wait()
    wide = x_ref[...].astype(F32)
    normalized = (wide * gain_ref[...]).astype(BF16)
    norm_ref[...] = normalized
    squares = jnp.sum(wide * wide, axis=1, keepdims=True)
    copies[2].wait()
    compressed = dot(normalized, down_ref[...])
    copies[3].wait()
    rope = dot(normalized, rope_ref[...], ((1,), (1,)))
    middle = rows // 2
    packed = jnp.concatenate([rope[:middle], rope[middle:]], axis=1)
    line = jnp.broadcast_to(squares, (rows, LANES)).T[:1]
    high = line.astype(BF16).astype(F32)
    own_ref[:rows] = compressed
    own_ref[rows : rows + middle] = packed
    own_ref[rows + middle :] = stacked(own_ref.shape[0] - rows - middle, [line])
    send_ref[:rows] = compressed.astype(BF16)
    send_ref[rows : rows + middle] = packed.astype(BF16)
    tail = stacked(own_ref.shape[0] - rows - middle, [high, line - high])
    send_ref[rows + middle :] = tail.astype(BF16)


def stacked(height, lines):
    row = lax.broadcasted_iota(jnp.int32, (height, LANES), 0)
    out = jnp.zeros((height, LANES), F32)
    count = 0
    for line in lines:
        for at in range(0, line.shape[1], LANES):
            out = jnp.where(row == count, line[:, at : at + LANES], out)
            count += 1
    return out


def turn(vectors, cosines, sines):
    half = vectors.shape[1] // 2
    swapped = jnp.concatenate([vectors[:, half:], vectors[:, :half]], axis=1)
    return vectors * cosines + swapped * sines


def latent_body(own_ref, got_ref, table_ref, gain_ref, block_ref, scale_ref, *, features):
    rows = scale_ref.shape[0]
    middle = rows // 2
    total = own_ref[...] + got_ref[...].astype(F32)
    compressed = total[:rows]
    packed = total[rows : rows + middle]
    tail = total[rows + middle :]
    count = rows // LANES
    squares = jnp.concatenate(
        [tail[k : k + 1] + tail[count + k : count + k + 1] for k in range(count)], axis=1
    )
    scale = jnp.broadcast_to(lax.rsqrt(squares / features + EPSILON), (LANES, rows)).T
    scale_ref[...] = scale
    mean = jnp.mean(compressed * compressed, axis=1, keepdims=True)
    block_ref[:rows] = (compressed * lax.rsqrt(mean + EPSILON) * gain_ref[...]).astype(BF16)
    rope = jnp.concatenate([packed[:, :D_ROPE], packed[:, D_ROPE:]], axis=0)
    rope = turn(rope * scale[:, :D_ROPE], table_ref[:, :D_ROPE], table_ref[:, D_ROPE:])
    block_ref[rows:] = jnp.concatenate([rope[:middle], rope[middle:]], axis=1).astype(BF16)


def stage_body(part_ref, w_ref, rest_ref, sem):
    half = rest_ref.shape[0]
    theirs = pl.multiple_of((1 - part_ref[0]) * half, half)
    copy = pltpu.make_async_copy(w_ref.at[pl.ds(theirs, half), :], rest_ref, sem)
    copy.start()
    copy.wait()


def own_body(offset_ref, part_ref, *refs, count):
    *refs, sems = refs
    weights = refs[:count]
    own_ref, table_ref = refs[count : count + 2]
    sums = refs[count + 2 : 2 * count + 2]
    rests = refs[2 * count + 2 : 3 * count + 1]
    mines = refs[3 * count + 1 :]
    half = own_ref.shape[1]
    part = part_ref[0]
    mine = pl.multiple_of(part * half, half)
    theirs = pl.multiple_of((1 - part) * half, half)
    first = [
        pltpu.make_async_copy(w.at[pl.ds(mine, half), :], m, sems.at[0, i])
        for i, (w, m) in enumerate(zip(weights, mines))
    ]
    second = [
        pltpu.make_async_copy(w.at[pl.ds(theirs, half), :], r, sems.at[1, i])
        for i, (w, r) in enumerate(zip(weights, rests))
    ]
    for copy in first + second:
        copy.start()
    row = lax.broadcasted_iota(jnp.int32, table_ref.shape, 0) + offset_ref[0]
    lane = lax.broadcasted_iota(jnp.int32, table_ref.shape, 1)
    turn_of = lane % (D_ROPE // 2)
    rate = jnp.exp2(turn_of.astype(F32) * (-2.0 / D_ROPE * np.log2(ROPE_BASE)))
    angle = row.astype(F32) * rate
    sine = jnp.sin(angle)
    sine = jnp.where(lane < D_ROPE + D_ROPE // 2, -sine, sine)
    table_ref[...] = jnp.where(lane < D_ROPE, jnp.cos(angle), sine)
    own = own_ref[...]
    for copy, mine_ref, sum_ref in zip(first, mines, sums):
        copy.wait()
        sum_ref[...] = dot(own, mine_ref[...])
    for copy in second:
        copy.wait()


def project_body(
    parity_ref, got_ref, scale_ref, table_ref, sk_ref, sv_ref, sq_ref, sl_ref, wk_ref, wv_ref, wq_ref, wl_ref,
    up_ref, q_ref, kv_ref, in_ref, out_ref, qa_ref, qb_ref,
):
    got = got_ref[...]
    rows = got.shape[0]
    row_scale = scale_ref[:, :1]

    def project(sum_ref, w_ref):
        return (sum_ref[...] + dot(got, w_ref[...])) * row_scale

    width = wk_ref.shape[1]
    kv_ref[:, :width] = project(sk_ref, wk_ref).astype(BF16)
    kv_ref[:, width:] = project(sv_ref, wv_ref).astype(BF16)
    even = parity_ref[0] == 0
    head = kv_ref[:WINDOW]
    tail = kv_ref[rows - WINDOW :]
    in_ref[...] = jnp.where(even, tail, head)
    out_ref[...] = jnp.where(even, head, tail)
    win = (project(sq_ref, wq_ref) * (DH**-0.5 * LOG2E)).astype(BF16)
    queries = project(sl_ref, wl_ref)
    step = UNROTATED_WIDTH + D_ROPE
    scale = step**-0.5 * LOG2E
    row = lax.broadcasted_iota(jnp.int32, (LANES, LANES), 0)
    col = lax.broadcasted_iota(jnp.int32, (LANES, LANES), 1)
    unit = jnp.where(row == col, 1.0, 0.0).astype(BF16)
    blank = jnp.zeros((rows, LANES - D_ROPE), F32)
    chunks = qa_ref.shape[0]
    span = rows // chunks
    shared = LANES // DH
    group = win.shape[1] // width
    for g in range(width // DH):
        pair = dot(unit, win[:, g * group * DH : (g + 1) * group * DH], ((1,), (1,))).astype(BF16)
        spot = g % shared * DH
        for c in range(chunks):
            q_ref[c, g] = jnp.zeros(q_ref.shape[2:], BF16)
            for j in range(group):
                q_ref[c, g, spot : spot + DH, j * span : (j + 1) * span] = pair[
                    j * DH : (j + 1) * DH, c * span : (c + 1) * span
                ]
    lat = up_ref.shape[0]
    for head in range(wl_ref.shape[1] // step):
        plain = queries[:, head * step : head * step + UNROTATED_WIDTH].astype(BF16)
        up = up_ref[:, head * UNROTATED_WIDTH : (head + 1) * UNROTATED_WIDTH]
        low = (dot(up, plain, ((1,), (1,))) * scale).astype(BF16)
        turned = queries[:, head * step + UNROTATED_WIDTH : (head + 1) * step]
        turned = turn(turned, table_ref[:, :D_ROPE], table_ref[:, D_ROPE:]) * scale
        first = jnp.concatenate([turned, blank], axis=1).astype(BF16)
        second = jnp.concatenate([blank, turned], axis=1).astype(BF16)
        first = dot(unit, first, ((1,), (1,))).astype(BF16)
        second = dot(unit, second, ((1,), (1,))).astype(BF16)
        for c in range(chunks):
            cols = slice(head * span, (head + 1) * span)
            rowsl = slice(c * span, (c + 1) * span)
            qa_ref[c, :lat, cols] = low[:, rowsl]
            qb_ref[c, :lat, cols] = low[:, rowsl]
            qa_ref[c, lat:, cols] = first[:, rowsl]
            qb_ref[c, lat:, cols] = second[:, rowsl]


def attend(groups, qa, qb, state):
    rows = groups[0][0].shape[0] * 2 // 3
    half = rows // 2
    columns = qa.shape[1]
    steps = [(blocks, part, table) for blocks in groups for part, table in ((0, qa), (1, qb))]

    def keys_of(step):
        blocks, part, _ = step
        return jnp.concatenate([b[part * half : (part + 1) * half] for b in blocks], axis=0)

    def score_of(step):
        rope = jnp.concatenate([b[rows : rows + half] for b in step[0]], axis=0)
        return dot(jnp.concatenate([keys_of(step), rope], axis=1), step[2])

    peak, total, weighted = state
    coming = score_of(steps[0])
    for i, step in enumerate(steps):
        score = coming
        if i + 1 < len(steps):
            coming = score_of(steps[i + 1])
        top = jnp.max(score, axis=0, keepdims=True)
        if peak is not None:
            top = jnp.maximum(peak, top)
        weight = jnp.exp2(score - top)
        new_total = jnp.sum(weight.reshape(-1, 8, columns), axis=0)
        new_weighted = dot(keys_of(step), weight.astype(BF16), ((0,), (0,)))
        if peak is not None:
            factor = jnp.exp2(peak - top)
            new_total = total * factor + new_total
            new_weighted = weighted * factor + new_weighted
        peak, total, weighted = top, new_total, new_weighted
    return peak, total, weighted


def begin_body(chunk_ref, *refs, groups):
    chunk = chunk_ref[0]
    qa_ref, qb_ref, stat_ref, sum_ref = refs[sum(groups) :]
    blocks = list(refs[: sum(groups)])
    parts = [[blocks.pop(0) for _ in range(size)] for size in groups]
    peak, total, weighted = attend(parts, qa_ref[chunk], qb_ref[chunk], (None, None, None))
    stat_ref[:8] = jnp.broadcast_to(peak, total.shape)
    stat_ref[8:] = total
    sum_ref[...] = weighted


def finish_body(
    offset_ref, part_ref, chunk_ref, *refs, groups, seq_total,
):
    count = sum(groups)
    (
        qa_ref, qb_ref, stat_ref, sum_ref, sink_ref, q_ref, halo_ref, kv_ref, up_ref,
        ow_ref, ol_ref, send_ref, keep_ref, cat_ref, pad_ref,
    ) = refs[count:]
    chunk = chunk_ref[0]
    total, weighted = stat_ref[8:], sum_ref[...]
    if count:
        blocks = list(refs[:count])
        parts = [[blocks.pop(0) for _ in range(size)] for size in groups]
        state = (stat_ref[:1], total, weighted)
        _, total, weighted = attend(parts, qa_ref[chunk], qb_ref[chunk], state)
    mixed = (weighted / jnp.sum(total, axis=0, keepdims=True)).astype(BF16)
    span, columns = send_ref.shape[0], mixed.shape[1]
    heads_l = columns // span
    _, key_heads, lanes, width = q_ref.shape
    group = width // span
    shared = lanes // DH
    own_rows = kv_ref.shape[0]
    pad_ref[pl.ds(pl.multiple_of((1 - chunk) * WINDOW, WINDOW), own_rows), :] = kv_ref[...]
    pad_ref[pl.ds(pl.multiple_of(chunk * own_rows, WINDOW), WINDOW), :] = halo_ref[...]
    padded = pad_ref[...]
    offset = offset_ref[0]
    key_pos = lax.broadcasted_iota(jnp.int32, (span + 2 * WINDOW, span), 0) - WINDOW
    query_pos = lax.broadcasted_iota(jnp.int32, (span + 2 * WINDOW, span), 1)
    distance = jnp.abs(key_pos - query_pos)
    spot = key_pos + (offset + chunk * span)
    inside = (distance <= WINDOW) & (spot >= 0) & (spot < seq_total)
    distance = jnp.where(inside, distance.astype(F32), -MASKED)
    distance = jnp.concatenate([distance] * group, axis=1)
    values_at = kv_ref.shape[1] // 2

    def sinks_of(g):
        return jnp.concatenate(
            [sink_ref[g * group + j : g * group + j + 1] for j in range(group)], axis=1
        )

    def slopes_of(g):
        first = part_ref[0] * (key_heads * group) + g * group + 1
        heads = first + lax.broadcasted_iota(jnp.int32, (1, group * span), 1) // span
        return jnp.exp2(heads.astype(F32) * (-8.0 / HEADS_A)) * LOG2E

    def score_of(g):
        at = g // shared * lanes
        return dot(padded[:, at : at + lanes], q_ref[chunk, g])

    coming = score_of(0)
    for g in range(key_heads):
        score = coming
        if g + 1 < key_heads:
            coming = score_of(g + 1)
        at = values_at + g // shared * lanes
        score = score - slopes_of(g) * distance
        sink = sinks_of(g)
        top = jnp.maximum(jnp.max(score, axis=0, keepdims=True), sink)
        weight = jnp.exp2(score - top)
        total = jnp.sum(weight, axis=0, keepdims=True) + jnp.exp2(sink - top)
        out = dot(padded[:, at : at + lanes], weight.astype(BF16), ((0,), (0,)))
        row = g % shared * DH
        out = (out[row : row + DH] / total).astype(BF16)
        for j in range(group):
            head = g * group + j
            cat_ref[head * DH : (head + 1) * DH, :] = out[:, j * span : (j + 1) * span]
    base = key_heads * group * DH
    for head in range(heads_l):
        up = up_ref[:, head * VALUE_WIDTH : (head + 1) * VALUE_WIDTH]
        out = dot(up, mixed[:, head * span : (head + 1) * span], ((0,), (0,)))
        cat_ref[base + head * VALUE_WIDTH : base + (head + 1) * VALUE_WIDTH, :] = out.astype(BF16)
    keep = keep_ref.shape[1]
    win = cat_ref[:base, :]
    low = cat_ref[base:, :]

    def out_of(start):
        return dot(win, ow_ref[:, start : start + keep], ((0,), (0,))) + dot(
            low, ol_ref[:, start : start + keep], ((0,), (0,))
        )

    first = out_of(0)
    second = out_of(keep)
    lower = part_ref[0] == 0
    send_ref[...] = jnp.where(lower, second, first).astype(BF16)
    keep_ref[...] = jnp.where(lower, first, second)


def store_body(chunk_ref, *refs, fresh):
    keep_ref, got_ref, out_ref, row_ref, sem = refs if fresh else refs[1:]
    span = keep_ref.shape[0]
    row_ref[...] = (keep_ref[...] + got_ref[...].astype(F32)).astype(BF16)
    place = pl.multiple_of(chunk_ref[0] * span, span)
    copy = pltpu.make_async_copy(row_ref, out_ref.at[pl.ds(place, span), :], sem)
    copy.start()
    copy.wait()


def store(chunk, keep, got, rows, whole_out=None):
    fresh = whole_out is None
    hbm = pl.BlockSpec(memory_space=pltpu.HBM)
    return pl.pallas_call(
        partial(store_body, fresh=fresh),
        out_shape=jax.ShapeDtypeStruct((rows, keep.shape[1]), BF16),
        in_specs=scalars(1) + ([] if fresh else [hbm]) + whole(2),
        out_specs=hbm,
        scratch_shapes=[pltpu.VMEM(keep.shape, BF16), pltpu.SemaphoreType.DMA],
        input_output_aliases={} if fresh else {1: 0},
        name="store" if fresh else "store_rest",
        compiler_params=pltpu.CompilerParams(vmem_limit_bytes=4 * 2**20),
    )(chunk[None], *([] if fresh else [whole_out]), keep, got)


def swap(cells, axis, bit):
    count = lax.axis_size(axis)
    return lax.ppermute(cells, axis, [(i, i ^ bit) for i in range(count)])


def gather(block):
    count = lax.axis_size("sp")
    if count % 4 or count > 16 or count & (count - 1):
        pieces = jnp.split(lax.all_gather(block, "sp", axis=0, tiled=True), count)
        return [pieces[: count // 2], pieces[count // 2 :]]
    line = [block] + [swap(block, "sp", 4 * k) for k in range(1, count // 4)]
    mine = line + [swap(b, "sp", 2) for b in line]
    across = [swap(b, "sp", 1) for b in mine]
    late = len(line) // 2
    early = len(mine) - late
    return [
        [*mine[:late], *across[:late], *mine[late:early], *across[late:early]],
        [*mine[early:], *across[early:]],
    ]


def per_device(
    activations,
    norm_gain,
    win_query,
    win_key,
    win_value,
    sink_logit,
    lat_query,
    key_value_down_weight,
    rope_key,
    latent_norm_gain,
    key_up_weight,
    value_up_weight,
    out_win,
    out_lat,
):
    rows, half = activations.shape
    features = norm_gain.shape[0]
    part = lax.axis_index("tp").astype(jnp.int32)
    count = lax.axis_size("sp")
    offset = lax.axis_index("sp").astype(jnp.int32) * rows
    shape = jax.ShapeDtypeStruct

    heads = sink_logit.shape[0]
    parity = lax.axis_index("sp").astype(jnp.int32) % 2
    flip = 1 - parity

    lat = key_value_down_weight.shape[1]
    height = rows + rows // 2 + 16
    normalized, own, send = call(
        compress_body,
        [shape((rows, half), BF16), shape((height, lat), F32), shape((height, lat), BF16)],
        [offset[None], part[None], parity[None], flip[None]], [activations, norm_gain[None], key_value_down_weight, rope_key.T], [],
        2 * rows * half * 192, 8,
        [
            pltpu.VMEM((rows, half), BF16),
            pltpu.VMEM((1, half), F32),
            pltpu.VMEM((half, lat), BF16),
            pltpu.VMEM((rope_key.shape[1], half), BF16),
            pltpu.SemaphoreType.DMA((4,)),
        ],
    )
    got = swap(send, "tp", 1)
    other = swap(normalized, "tp", 1)
    weights = [win_key, win_value, win_query, lat_query]
    table, *partial_sums = call(
        partial(own_body, count=len(weights)),
        [shape((rows, LANES), F32)] + [shape((rows, w.shape[1]), F32) for w in weights]
        + [shape((half, w.shape[1]), BF16) for w in weights[:-1]],
        [offset[None], part[None]], weights, [normalized],
        2 * rows * half * 1792, 16,
        [pltpu.VMEM((half, w.shape[1]), BF16) for w in weights]
        + [pltpu.SemaphoreType.DMA((2, len(weights)))],
    )
    staged = call(
        stage_body, shape((half, weights[-1].shape[1]), BF16),
        [part[None]], weights[-1:], [], 1e6, 4, [pltpu.SemaphoreType.DMA],
    )
    block, row_scale = call(
        partial(latent_body, features=features),
        [shape((rows + rows // 2, lat), BF16), shape((rows, LANES), F32)],
        [], [], [own, got, table, latent_norm_gain[None]],
        1e6, 4,
    )
    groups = gather(block)

    chunks = rows // WINDOW
    span = rows // chunks
    group = win_query.shape[1] // win_key.shape[1]
    columns = lat_query.shape[1] // (UNROTATED_WIDTH + D_ROPE) * (rows // chunks)
    queries, key_value, inward, outward, table_a, table_b = call(
        project_body,
        [
            shape((chunks, win_key.shape[1] // DH, LANES, group * span), BF16),
            shape((rows, win_key.shape[1] + win_value.shape[1]), BF16),
            shape((WINDOW, win_key.shape[1] + win_value.shape[1]), BF16),
            shape((WINDOW, win_key.shape[1] + win_value.shape[1]), BF16),
            shape((chunks, lat + LANES, columns), BF16),
            shape((chunks, lat + LANES, columns), BF16),
        ],
        [parity[None]], [],
        [other, row_scale, table, *partial_sums, staged, key_up_weight],
        2 * rows * half * 1792, 16,
    )
    inner = lax.ppermute(inward, "sp", [(i, i ^ 1) for i in range(count) if i ^ 1 < count])

    def partner(i):
        other = i + 1 if i % 2 else i - 1
        return other if 0 <= other < count else i

    outer = lax.ppermute(
        outward, "sp", [(i, partner(i)) for i in range(count)]
    )

    sinks = jnp.broadcast_to(sink_logit[:, None] * LOG2E, (heads, LANES))
    kept = []
    assert chunks == 2
    result = None
    order = (flip, parity)
    for c, (chunk, halo) in enumerate(zip(order, (inner, outer))):
        first = groups[:1] if c == 0 else groups
        last = groups[1:] if c == 0 else []
        sizes = []
        for g in first:
            sizes += [len(g) // 2, len(g) - len(g) // 2] if len(g) > 8 else [len(g)]
        state = call(
            partial(begin_body, groups=sizes),
            [shape((16, columns), F32), shape((lat, columns), F32)],
            [chunk[None]], [], [*(b for g in first for b in g), table_a, table_b], 3e9, 32,
        )
        send, keep = call(
            partial(finish_body, groups=[len(g) for g in last], seq_total=rows * count),
            [shape((span, half), BF16), shape((span, half), F32)],
            [offset[None], part[None], chunk[None]], [],
            [
                *(b for g in last for b in g), table_a, table_b, *state, sinks, queries, halo,
                key_value, value_up_weight, out_win, out_lat,
            ],
            1e9, 16,
            [
                pltpu.VMEM((out_win.shape[0] + out_lat.shape[0], span), BF16),
                pltpu.VMEM((rows + WINDOW, key_value.shape[1]), BF16),
            ],
        )
        kept.append((chunk, keep, swap(send, "tp", 1)))
    for chunk, keep, got in kept:
        result = store(chunk, keep, got, rows, result)
    return result


def solution(mesh):
    narrow = mesh.shape["tp"] == 2
    body = per_device if narrow else per_device_wide
    return jax.shard_map(
        body,
        mesh=mesh,
        in_specs=(
            P("sp", "tp"),
            P(),
            P(None, "tp"),
            P(None, "tp"),
            P(None, "tp"),
            P("tp"),
            P(None, "tp"),
            P(),
            P(),
            P(),
            P(None, "tp"),
            P(None, "tp"),
            P("tp", None),
            P("tp", None),
        ),
        out_specs=P("sp", "tp"),
        check_vma=False,
    )
```

```python
from functools import partial

import jax
import jax.numpy as jnp
import numpy as np
from jax import lax
from jax.experimental import pallas as pl
from jax.experimental.pallas import tpu as pltpu
from jax.sharding import PartitionSpec as P


HEADS_A = 16
DH = 64
WINDOW = 128
UNROTATED_WIDTH = 128
D_ROPE = 64
VALUE_WIDTH = 128


EPSILON = 1e-06
ROPE_BASE = 10000.0
LOG2E = 1.4426950408889634
LANES = 128
MASKED = -1e30


F32 = jnp.float32
BF16 = jnp.bfloat16


def padded_2(cells, sides, width):
    for axis, dim in sides:
        count = lax.axis_size(axis)
        ends = count - 1
        head = lax.slice_in_dim(cells, 0, width, axis=dim)
        tail = lax.slice_in_dim(cells, cells.shape[dim] - width, cells.shape[dim], axis=dim)
        cells = jnp.concatenate(
            [
                lax.ppermute(tail, axis, [(i, (i + 1) % count) for i in range(ends)]),
                cells,
                lax.ppermute(head, axis, [((i + 1) % count, i) for i in range(ends)]),
            ],
            axis=dim,
        )
    return cells


def rotate(vectors, angles):
    half_width = vectors.shape[-1] // 2
    cosine_table = jnp.cos(angles)
    sine_table = jnp.sin(angles)
    lower_half = vectors[..., :half_width]
    upper_half = vectors[..., half_width:]
    return jnp.concatenate(
        [
            lower_half * cosine_table - upper_half * sine_table,
            lower_half * sine_table + upper_half * cosine_table,
        ],
        axis=-1,
    )


def rotary_angles(places, width):
    frequency = 1.0 / ROPE_BASE ** (jnp.arange(0, width, 2).astype(jnp.float32) / width)
    return places[:, None] * frequency[None, :]


def window_attention(queries, padded, sinks, offset, seq_total, head_start):
    tok_rows = queries.shape[0]
    key_heads = padded.shape[1] // (2 * DH)
    groups = queries.shape[1] // (DH * key_heads)
    key_rows = padded[:, : key_heads * DH].reshape(-1, key_heads, DH)
    value_rows = padded[:, key_heads * DH :].reshape(-1, key_heads, DH)
    grouped = queries.reshape(tok_rows, key_heads, groups, DH)
    scores = jnp.einsum(
        "qhgd,khd->hgqk", grouped, key_rows, preferred_element_type=jnp.float32
    ) * DH ** (-0.5)
    query_pos = offset + jnp.arange(tok_rows, dtype=jnp.int32)
    key_pos = offset - WINDOW + jnp.arange(tok_rows + 2 * WINDOW, dtype=jnp.int32)
    distance = jnp.abs(query_pos[:, None] - key_pos[None, :])
    in_window = (distance <= WINDOW) & (key_pos[None, :] >= 0) & (key_pos[None, :] < seq_total)
    head_ids = head_start + jnp.arange(key_heads * groups, dtype=jnp.int32)
    slopes = jnp.exp2(-8.0 * (head_ids + 1).astype(jnp.float32) / HEADS_A).reshape(
        key_heads, groups
    )
    scores = scores - slopes[:, :, None, None] * distance.astype(jnp.float32)[None, None]
    scores = jnp.where(in_window[None, None], scores, -jnp.inf)
    sink_table = sinks.reshape(key_heads, groups)
    row_peak = jnp.maximum(jnp.max(scores, axis=3), sink_table[:, :, None])
    weights = jnp.exp(scores - row_peak[..., None])
    denominator = jnp.sum(weights, axis=3) + jnp.exp(sink_table[:, :, None] - row_peak)
    blended = jnp.einsum(
        "hgqk,khd->qhgd",
        weights.astype(jnp.bfloat16),
        value_rows,
        preferred_element_type=jnp.float32,
    )
    blended = blended / jnp.transpose(denominator, (2, 0, 1))[..., None]
    return blended.reshape(tok_rows, key_heads * groups * DH).astype(jnp.bfloat16)


def latent_step(running, key_block, query_plain, query_turned):
    row_peak, totals, weighted = running
    keys_plain, values_plain, keys_turned = key_block
    key_count = keys_plain.shape[0]
    head_count = query_plain.shape[1]
    scores = jnp.einsum(
        "qhd,khd->hqk",
        query_plain,
        keys_plain.reshape(key_count, head_count, UNROTATED_WIDTH),
        preferred_element_type=jnp.float32,
    )
    scores = scores + jnp.einsum(
        "qhd,kd->hqk", query_turned, keys_turned, preferred_element_type=jnp.float32
    )
    scores = scores * (UNROTATED_WIDTH + D_ROPE) ** (-0.5)
    new_peak = jnp.maximum(row_peak, jnp.max(scores, axis=2))
    factor = jnp.exp(row_peak - new_peak)
    weights = jnp.exp(scores - new_peak[..., None])
    totals = totals * factor + jnp.sum(weights, axis=2)
    weighted = weighted * factor[..., None] + jnp.einsum(
        "hqk,khd->hqd",
        weights.astype(jnp.bfloat16),
        values_plain.reshape(key_count, head_count, VALUE_WIDTH),
        preferred_element_type=jnp.float32,
    )
    return (new_peak, totals, weighted)


def over_blocks(running, pieces, prepare, attend, block_rows):
    key_count = pieces[0].shape[0]
    stacked = tuple(
        (
            piece_part.reshape((key_count // block_rows, block_rows) + piece_part.shape[1:])
            for piece_part in pieces
        )
    )

    def one_block(state_now, key_block):
        return (attend(state_now, prepare(key_block)), None)

    return lax.scan(one_block, running, stacked)[0]


def per_device_wide(
    activations,
    norm_gain,
    win_query,
    win_key,
    win_value,
    sink_logit,
    lat_query,
    key_value_down_weight,
    rope_key,
    latent_norm_gain,
    key_up_weight,
    value_up_weight,
    out_win,
    out_lat,
):
    tok_rows = activations.shape[0]
    weights_all = (win_query, win_key, win_value, lat_query, key_value_down_weight, rope_key)
    widened = lax.all_gather(activations, "tp", axis=1, tiled=True).astype(jnp.float32)
    normalized = (widened * norm_gain[None, :]).astype(jnp.bfloat16)
    squares = jnp.sum(widened * widened, axis=1)
    totals = tuple(
        (jnp.dot(normalized, weight, preferred_element_type=jnp.float32) for weight in weights_all)
    )
    squares, totals = (squares, totals)
    win_proj, key_proj, value_proj, latq_proj, compressed, rope_proj = totals
    row_scale = lax.rsqrt(squares / norm_gain.shape[0] + EPSILON)[:, None]
    offset = lax.axis_index("sp") * tok_rows
    seq_total = tok_rows * lax.axis_size("sp")
    places = (offset + jnp.arange(tok_rows, dtype=jnp.int32)).astype(jnp.float32)
    angles = rotary_angles(places, D_ROPE)
    win_queries = (win_proj * row_scale).astype(jnp.bfloat16)
    key_value = jnp.concatenate(
        [
            (key_proj * row_scale).astype(jnp.bfloat16),
            (value_proj * row_scale).astype(jnp.bfloat16),
        ],
        axis=1,
    )
    padded = padded_2(key_value, (("sp", 0),), WINDOW)
    head_start = lax.axis_index("tp") * sink_logit.shape[0]
    win_out = window_attention(win_queries, padded, sink_logit, offset, seq_total, head_start)
    head_count = lat_query.shape[1] // (UNROTATED_WIDTH + D_ROPE)
    query_all = (latq_proj * row_scale).reshape(tok_rows, head_count, UNROTATED_WIDTH + D_ROPE)
    query_plain = query_all[..., :UNROTATED_WIDTH].astype(jnp.bfloat16)
    query_turned = rotate(query_all[..., UNROTATED_WIDTH:], angles[:, None, :]).astype(jnp.bfloat16)
    latent = (
        compressed
        * lax.rsqrt(jnp.mean(compressed * compressed, axis=1, keepdims=True) + EPSILON)
        * latent_norm_gain[None, :]
    ).astype(jnp.bfloat16)
    key_rotary = rotate(rope_proj * row_scale, angles).astype(jnp.bfloat16)
    attend = partial(latent_step, query_plain=query_plain, query_turned=query_turned)

    def expand(key_block):
        return (
            jnp.dot(key_block[0], key_up_weight, preferred_element_type=jnp.float32).astype(
                jnp.bfloat16
            ),
            jnp.dot(key_block[0], value_up_weight, preferred_element_type=jnp.float32).astype(
                jnp.bfloat16
            ),
            key_block[1],
        )

    _, totals_lat, weighted = over_blocks(
        (
            jnp.full((head_count, tok_rows), -jnp.inf, jnp.float32),
            jnp.zeros((head_count, tok_rows), jnp.float32),
            jnp.zeros((head_count, tok_rows, VALUE_WIDTH), jnp.float32),
        ),
        (
            lax.all_gather(latent, "sp", axis=0, tiled=True),
            lax.all_gather(key_rotary, "sp", axis=0, tiled=True),
        ),
        expand,
        attend,
        2048,
    )
    lat_out = (
        (weighted / totals_lat[..., None])
        .transpose(1, 0, 2)
        .reshape(tok_rows, head_count * VALUE_WIDTH)
    )
    lat_out = lat_out.astype(jnp.bfloat16)
    terms = jnp.dot(win_out, out_win, preferred_element_type=jnp.float32) + jnp.dot(
        lat_out, out_lat, preferred_element_type=jnp.float32
    )
    return lax.psum_scatter(terms.astype(jnp.bfloat16), "tp", scatter_dimension=1, tiled=True)


def dot(a, b, dims=((1,), (0,))):
    return lax.dot_general(a, b, (dims, ((), ())), preferred_element_type=F32)


def whole(count):
    return [pl.BlockSpec(memory_space=pltpu.VMEM)] * count


def scalars(count):
    return [pl.BlockSpec(memory_space=pltpu.SMEM)] * count


def call(body, shapes, smem, hbm, operands, flops, mib, scratch=()):
    single = not isinstance(shapes, (list, tuple))
    outs = [shapes] if single else list(shapes)
    result = pl.pallas_call(
        body,
        out_shape=outs,
        in_specs=scalars(len(smem))
        + [pl.BlockSpec(memory_space=pltpu.HBM)] * len(hbm)
        + whole(len(operands)),
        out_specs=whole(len(outs)),
        scratch_shapes=list(scratch),
        cost_estimate=pl.CostEstimate(
            flops=int(flops),
            bytes_accessed=sum(x.size * x.dtype.itemsize for x in [*hbm, *operands]),
            transcendentals=0,
        ),
        compiler_params=pltpu.CompilerParams(vmem_limit_bytes=mib * 2**20),
    )(*smem, *[pltpu.with_memory_space_constraint(x, pltpu.HBM) for x in hbm], *operands)
    return result[0] if single else result


def compress_body(
    offset_ref, part_ref, parity_ref, other_ref, x_hbm, gain_hbm, down_hbm, rope_hbm, norm_ref, own_ref, send_ref,
    x_ref, gain_ref, down_ref, rope_ref, sems,
):
    rows, half = x_hbm.shape
    del offset_ref, parity_ref, other_ref
    start = pl.multiple_of(part_ref[0] * half, half)
    middle = rows // 2
    copies = [
        pltpu.make_async_copy(x_hbm.at[:middle], x_ref.at[:middle], sems.at[0]),
        pltpu.make_async_copy(gain_hbm.at[:, pl.ds(start, half)], gain_ref, sems.at[3]),
        pltpu.make_async_copy(down_hbm.at[pl.ds(start, half), :], down_ref, sems.at[1]),
        pltpu.make_async_copy(rope_hbm.at[:, pl.ds(start, half)], rope_ref, sems.at[2]),
    ]
    copies.append(pltpu.make_async_copy(x_hbm.at[middle:], x_ref.at[middle:], sems.at[4]))
    for copy in copies:
        copy.start()
    copies[1].wait()
    parts = []
    for at, copy in ((0, copies[0]), (middle, copies[4])):
        copy.wait()
        wide = x_ref[at : at + middle].astype(F32)
        normalized = (wide * gain_ref[...]).astype(BF16)
        norm_ref[at : at + middle] = normalized
        squares = jnp.sum(wide * wide, axis=1, keepdims=True)
        if at == 0:
            copies[2].wait()
            copies[3].wait()
        compressed = dot(normalized, down_ref[...])
        parts.append((squares, compressed, dot(normalized, rope_ref[...], ((1,), (1,)))))
    squares, compressed, rope = (jnp.concatenate(p, axis=0) for p in zip(*parts))
    packed = jnp.concatenate([rope[:middle], rope[middle:]], axis=1)
    line = jnp.broadcast_to(squares, (rows, LANES)).T[:1]
    high = line.astype(BF16).astype(F32)
    own_ref[:rows] = compressed
    own_ref[rows : rows + middle] = packed
    own_ref[rows + middle :] = stacked(own_ref.shape[0] - rows - middle, [line])
    send_ref[:rows] = compressed.astype(BF16)
    send_ref[rows : rows + middle] = packed.astype(BF16)
    tail = stacked(own_ref.shape[0] - rows - middle, [high, line - high])
    send_ref[rows + middle :] = tail.astype(BF16)


def stacked(height, lines):
    row = lax.broadcasted_iota(jnp.int32, (height, LANES), 0)
    out = jnp.zeros((height, LANES), F32)
    count = 0
    for line in lines:
        for at in range(0, line.shape[1], LANES):
            out = jnp.where(row == count, line[:, at : at + LANES], out)
            count += 1
    return out


def turn(vectors, cosines, sines):
    half = vectors.shape[1] // 2
    swapped = jnp.concatenate([vectors[:, half:], vectors[:, :half]], axis=1)
    return vectors * cosines + swapped * sines


def latent_body(own_ref, got_ref, table_ref, gain_ref, block_ref, scale_ref, *, features):
    rows = scale_ref.shape[0]
    middle = rows // 2
    total = own_ref[...] + got_ref[...].astype(F32)
    compressed = total[:rows]
    packed = total[rows : rows + middle]
    tail = total[rows + middle :]
    count = rows // LANES
    squares = jnp.concatenate(
        [tail[k : k + 1] + tail[count + k : count + k + 1] for k in range(count)], axis=1
    )
    scale = jnp.broadcast_to(lax.rsqrt(squares / features + EPSILON), (LANES, rows)).T
    scale_ref[...] = scale
    mean = jnp.mean(compressed * compressed, axis=1, keepdims=True)
    block_ref[:rows] = (compressed * lax.rsqrt(mean + EPSILON) * gain_ref[...]).astype(BF16)
    rope = jnp.concatenate([packed[:, :D_ROPE], packed[:, D_ROPE:]], axis=0)
    rope = turn(rope * scale[:, :D_ROPE], table_ref[:, :D_ROPE], table_ref[:, D_ROPE:])
    block_ref[rows:] = jnp.concatenate([rope[:middle], rope[middle:]], axis=1).astype(BF16)


def stage_body(part_ref, w_ref, rest_ref, sem):
    half = rest_ref.shape[0]
    theirs = pl.multiple_of((1 - part_ref[0]) * half, half)
    copy = pltpu.make_async_copy(w_ref.at[pl.ds(theirs, half), :], rest_ref, sem)
    copy.start()
    copy.wait()


def own_body(offset_ref, part_ref, *refs, count):
    *refs, sems = refs
    weights = refs[:count]
    own_ref, table_ref = refs[count : count + 2]
    sums = refs[count + 2 : 2 * count + 2]
    rests = refs[2 * count + 2 : 3 * count + 1]
    mines = refs[3 * count + 1 :]
    half = own_ref.shape[1]
    part = part_ref[0]
    mine = pl.multiple_of(part * half, half)
    theirs = pl.multiple_of((1 - part) * half, half)
    first = [
        pltpu.make_async_copy(w.at[pl.ds(mine, half), :], m, sems.at[0, i])
        for i, (w, m) in enumerate(zip(weights, mines))
    ]
    second = [
        pltpu.make_async_copy(w.at[pl.ds(theirs, half), :], r, sems.at[1, i])
        for i, (w, r) in enumerate(zip(weights, rests))
    ]
    for copy in first + second:
        copy.start()
    row = lax.broadcasted_iota(jnp.int32, table_ref.shape, 0) + offset_ref[0]
    lane = lax.broadcasted_iota(jnp.int32, table_ref.shape, 1)
    turn_of = lane % (D_ROPE // 2)
    rate = jnp.exp2(turn_of.astype(F32) * (-2.0 / D_ROPE * np.log2(ROPE_BASE)))
    angle = row.astype(F32) * rate
    sine = jnp.sin(angle)
    sine = jnp.where(lane < D_ROPE + D_ROPE // 2, -sine, sine)
    table_ref[...] = jnp.where(lane < D_ROPE, jnp.cos(angle), sine)
    own = own_ref[...]
    for copy, mine_ref, sum_ref in zip(first, mines, sums):
        copy.wait()
        sum_ref[...] = dot(own, mine_ref[...])
    for copy in second:
        copy.wait()


def project_body(
    parity_ref, got_ref, scale_ref, table_ref, sk_ref, sv_ref, sq_ref, sl_ref, wk_ref, wv_ref, wq_ref, wl_ref,
    up_ref, q_ref, kv_ref, in_ref, out_ref, qa_ref, qb_ref,
):
    got = got_ref[...]
    rows = got.shape[0]
    row_scale = scale_ref[:, :1]

    def project(sum_ref, w_ref):
        return (sum_ref[...] + dot(got, w_ref[...])) * row_scale

    width = wk_ref.shape[1]
    kv_ref[:, :width] = project(sk_ref, wk_ref).astype(BF16)
    kv_ref[:, width:] = project(sv_ref, wv_ref).astype(BF16)
    even = parity_ref[0] == 0
    head = kv_ref[:WINDOW]
    tail = kv_ref[rows - WINDOW :]
    in_ref[...] = jnp.where(even, tail, head)
    out_ref[...] = jnp.where(even, head, tail)
    win = (project(sq_ref, wq_ref) * (DH**-0.5 * LOG2E)).astype(BF16)
    queries = project(sl_ref, wl_ref)
    step = UNROTATED_WIDTH + D_ROPE
    scale = step**-0.5 * LOG2E
    row = lax.broadcasted_iota(jnp.int32, (LANES, LANES), 0)
    col = lax.broadcasted_iota(jnp.int32, (LANES, LANES), 1)
    unit = jnp.where(row == col, 1.0, 0.0).astype(BF16)
    blank = jnp.zeros((rows, LANES - D_ROPE), F32)
    chunks = qa_ref.shape[0]
    span = rows // chunks
    shared = LANES // DH
    group = win.shape[1] // width
    for g in range(width // DH):
        pair = dot(unit, win[:, g * group * DH : (g + 1) * group * DH], ((1,), (1,))).astype(BF16)
        spot = g % shared * DH
        for c in range(chunks):
            q_ref[c, g] = jnp.zeros(q_ref.shape[2:], BF16)
            for j in range(group):
                q_ref[c, g, spot : spot + DH, j * span : (j + 1) * span] = pair[
                    j * DH : (j + 1) * DH, c * span : (c + 1) * span
                ]
    lat = up_ref.shape[0]
    for head in range(wl_ref.shape[1] // step):
        plain = queries[:, head * step : head * step + UNROTATED_WIDTH].astype(BF16)
        up = up_ref[:, head * UNROTATED_WIDTH : (head + 1) * UNROTATED_WIDTH]
        low = (dot(up, plain, ((1,), (1,))) * scale).astype(BF16)
        turned = queries[:, head * step + UNROTATED_WIDTH : (head + 1) * step]
        turned = turn(turned, table_ref[:, :D_ROPE], table_ref[:, D_ROPE:]) * scale
        first = jnp.concatenate([turned, blank], axis=1).astype(BF16)
        second = jnp.concatenate([blank, turned], axis=1).astype(BF16)
        first = dot(unit, first, ((1,), (1,))).astype(BF16)
        second = dot(unit, second, ((1,), (1,))).astype(BF16)
        for c in range(chunks):
            cols = slice(head * span, (head + 1) * span)
            rowsl = slice(c * span, (c + 1) * span)
            qa_ref[c, :lat, cols] = low[:, rowsl]
            qb_ref[c, :lat, cols] = low[:, rowsl]
            qa_ref[c, lat:, cols] = first[:, rowsl]
            qb_ref[c, lat:, cols] = second[:, rowsl]


def attend(groups, qa, qb, state):
    rows = groups[0][0].shape[0] * 2 // 3
    half = rows // 2
    columns = qa.shape[1]
    steps = [(blocks, part, table) for blocks in groups for part, table in ((0, qa), (1, qb))]

    def keys_of(step):
        blocks, part, _ = step
        return jnp.concatenate([b[part * half : (part + 1) * half] for b in blocks], axis=0)

    def score_of(step):
        rope = jnp.concatenate([b[rows : rows + half] for b in step[0]], axis=0)
        return dot(jnp.concatenate([keys_of(step), rope], axis=1), step[2])

    peak, total, weighted = state
    coming = score_of(steps[0])
    for i, step in enumerate(steps):
        score = coming
        if i + 1 < len(steps):
            coming = score_of(steps[i + 1])
        top = jnp.max(score, axis=0, keepdims=True)
        if peak is not None:
            top = jnp.maximum(peak, top)
        weight = jnp.exp2(score - top)
        new_total = jnp.sum(weight.reshape(-1, 8, columns), axis=0)
        new_weighted = dot(keys_of(step), weight.astype(BF16), ((0,), (0,)))
        if peak is not None:
            factor = jnp.exp2(peak - top)
            new_total = total * factor + new_total
            new_weighted = weighted * factor + new_weighted
        peak, total, weighted = top, new_total, new_weighted
    return peak, total, weighted


def begin_body(chunk_ref, *refs, groups):
    chunk = chunk_ref[0]
    qa_ref, qb_ref, stat_ref, sum_ref = refs[sum(groups) :]
    blocks = list(refs[: sum(groups)])
    parts = [[blocks.pop(0) for _ in range(size)] for size in groups]
    peak, total, weighted = attend(parts, qa_ref[chunk], qb_ref[chunk], (None, None, None))
    stat_ref[:8] = jnp.broadcast_to(peak, total.shape)
    stat_ref[8:] = total
    sum_ref[...] = weighted


def finish_body(
    offset_ref, part_ref, chunk_ref, *refs, groups, seq_total,
):
    count = sum(groups)
    (
        qa_ref, qb_ref, stat_ref, sum_ref, sink_ref, q_ref, halo_ref, kv_ref, up_ref,
        ow_ref, ol_ref, send_ref, keep_ref, cat_ref, pad_ref,
    ) = refs[count:]
    chunk = chunk_ref[0]
    total, weighted = stat_ref[8:], sum_ref[...]
    if count:
        blocks = list(refs[:count])
        parts = [[blocks.pop(0) for _ in range(size)] for size in groups]
        state = (stat_ref[:1], total, weighted)
        _, total, weighted = attend(parts, qa_ref[chunk], qb_ref[chunk], state)
    mixed = (weighted / jnp.sum(total, axis=0, keepdims=True)).astype(BF16)
    span, columns = send_ref.shape[0], mixed.shape[1]
    heads_l = columns // span
    _, key_heads, lanes, width = q_ref.shape
    group = width // span
    shared = lanes // DH
    own_rows = kv_ref.shape[0]
    pad_ref[pl.ds(pl.multiple_of((1 - chunk) * WINDOW, WINDOW), own_rows), :] = kv_ref[...]
    pad_ref[pl.ds(pl.multiple_of(chunk * own_rows, WINDOW), WINDOW), :] = halo_ref[...]
    padded = pad_ref[...]
    offset = offset_ref[0]
    key_pos = lax.broadcasted_iota(jnp.int32, (span + 2 * WINDOW, span), 0) - WINDOW
    query_pos = lax.broadcasted_iota(jnp.int32, (span + 2 * WINDOW, span), 1)
    distance = jnp.abs(key_pos - query_pos)
    spot = key_pos + (offset + chunk * span)
    inside = (distance <= WINDOW) & (spot >= 0) & (spot < seq_total)
    distance = jnp.where(inside, distance.astype(F32), -MASKED)
    distance = jnp.concatenate([distance] * group, axis=1)
    values_at = kv_ref.shape[1] // 2

    def sinks_of(g):
        return jnp.concatenate(
            [sink_ref[g * group + j : g * group + j + 1] for j in range(group)], axis=1
        )

    def slopes_of(g):
        first = part_ref[0] * (key_heads * group) + g * group + 1
        heads = first + lax.broadcasted_iota(jnp.int32, (1, group * span), 1) // span
        return jnp.exp2(heads.astype(F32) * (-8.0 / HEADS_A)) * LOG2E

    def score_of(g):
        at = g // shared * lanes
        return dot(padded[:, at : at + lanes], q_ref[chunk, g])

    coming = score_of(0)
    for g in range(key_heads):
        score = coming
        if g + 1 < key_heads:
            coming = score_of(g + 1)
        at = values_at + g // shared * lanes
        score = score - slopes_of(g) * distance
        sink = sinks_of(g)
        top = jnp.maximum(jnp.max(score, axis=0, keepdims=True), sink)
        weight = jnp.exp2(score - top)
        total = jnp.sum(weight, axis=0, keepdims=True) + jnp.exp2(sink - top)
        out = dot(padded[:, at : at + lanes], weight.astype(BF16), ((0,), (0,)))
        row = g % shared * DH
        out = (out[row : row + DH] / total).astype(BF16)
        for j in range(group):
            head = g * group + j
            cat_ref[head * DH : (head + 1) * DH, :] = out[:, j * span : (j + 1) * span]
    base = key_heads * group * DH
    for head in range(heads_l):
        up = up_ref[:, head * VALUE_WIDTH : (head + 1) * VALUE_WIDTH]
        out = dot(up, mixed[:, head * span : (head + 1) * span], ((0,), (0,)))
        cat_ref[base + head * VALUE_WIDTH : base + (head + 1) * VALUE_WIDTH, :] = out.astype(BF16)
    keep = keep_ref.shape[1]
    win = cat_ref[:base, :]
    low = cat_ref[base:, :]

    def out_of(start):
        return dot(win, ow_ref[:, start : start + keep], ((0,), (0,))) + dot(
            low, ol_ref[:, start : start + keep], ((0,), (0,))
        )

    first = out_of(0)
    second = out_of(keep)
    lower = part_ref[0] == 0
    send_ref[...] = jnp.where(lower, second, first).astype(BF16)
    keep_ref[...] = jnp.where(lower, first, second)


def store_body(chunk_ref, *refs, fresh):
    keep_ref, got_ref, out_ref, row_ref, sem = refs if fresh else refs[1:]
    span = keep_ref.shape[0]
    row_ref[...] = (keep_ref[...] + got_ref[...].astype(F32)).astype(BF16)
    place = pl.multiple_of(chunk_ref[0] * span, span)
    copy = pltpu.make_async_copy(row_ref, out_ref.at[pl.ds(place, span), :], sem)
    copy.start()
    copy.wait()


def store(chunk, keep, got, rows, whole_out=None):
    fresh = whole_out is None
    hbm = pl.BlockSpec(memory_space=pltpu.HBM)
    return pl.pallas_call(
        partial(store_body, fresh=fresh),
        out_shape=jax.ShapeDtypeStruct((rows, keep.shape[1]), BF16),
        in_specs=scalars(1) + ([] if fresh else [hbm]) + whole(2),
        out_specs=hbm,
        scratch_shapes=[pltpu.VMEM(keep.shape, BF16), pltpu.SemaphoreType.DMA],
        input_output_aliases={} if fresh else {1: 0},
        name="store" if fresh else "store_rest",
        compiler_params=pltpu.CompilerParams(vmem_limit_bytes=4 * 2**20),
    )(chunk[None], *([] if fresh else [whole_out]), keep, got)


def swap(cells, axis, bit):
    count = lax.axis_size(axis)
    return lax.ppermute(cells, axis, [(i, i ^ bit) for i in range(count)])


def gather(block):
    count = lax.axis_size("sp")
    if count % 4 or count > 16 or count & (count - 1):
        pieces = jnp.split(lax.all_gather(block, "sp", axis=0, tiled=True), count)
        return [pieces[: count // 2], pieces[count // 2 :]]
    line = [block] + [swap(block, "sp", 4 * k) for k in range(1, count // 4)]
    mine = line + [swap(b, "sp", 2) for b in line]
    across = [swap(b, "sp", 1) for b in mine]
    late = len(line) // 2
    early = len(mine) - late
    return [
        [*mine[:late], *across[:late], *mine[late:early], *across[late:early]],
        [*mine[early:], *across[early:]],
    ]


def per_device(
    activations,
    norm_gain,
    win_query,
    win_key,
    win_value,
    sink_logit,
    lat_query,
    key_value_down_weight,
    rope_key,
    latent_norm_gain,
    key_up_weight,
    value_up_weight,
    out_win,
    out_lat,
):
    rows, half = activations.shape
    features = norm_gain.shape[0]
    part = lax.axis_index("tp").astype(jnp.int32)
    count = lax.axis_size("sp")
    offset = lax.axis_index("sp").astype(jnp.int32) * rows
    shape = jax.ShapeDtypeStruct

    heads = sink_logit.shape[0]
    parity = lax.axis_index("sp").astype(jnp.int32) % 2
    flip = 1 - parity

    lat = key_value_down_weight.shape[1]
    height = rows + rows // 2 + 16
    normalized, own, send = call(
        compress_body,
        [shape((rows, half), BF16), shape((height, lat), F32), shape((height, lat), BF16)],
        [offset[None], part[None], parity[None], flip[None]], [activations, norm_gain[None], key_value_down_weight, rope_key.T], [],
        2 * rows * half * 192, 8,
        [
            pltpu.VMEM((rows, half), BF16),
            pltpu.VMEM((1, half), F32),
            pltpu.VMEM((half, lat), BF16),
            pltpu.VMEM((rope_key.shape[1], half), BF16),
            pltpu.SemaphoreType.DMA((5,)),
        ],
    )
    got = swap(send, "tp", 1)
    other = swap(normalized, "tp", 1)
    weights = [win_key, win_value, win_query, lat_query]
    table, *partial_sums = call(
        partial(own_body, count=len(weights)),
        [shape((rows, LANES), F32)] + [shape((rows, w.shape[1]), F32) for w in weights]
        + [shape((half, w.shape[1]), BF16) for w in weights[:-1]],
        [offset[None], part[None]], weights, [normalized],
        2 * rows * half * 1792, 16,
        [pltpu.VMEM((half, w.shape[1]), BF16) for w in weights]
        + [pltpu.SemaphoreType.DMA((2, len(weights)))],
    )
    staged = call(
        stage_body, shape((half, weights[-1].shape[1]), BF16),
        [part[None]], weights[-1:], [], 1e6, 4, [pltpu.SemaphoreType.DMA],
    )
    block, row_scale = call(
        partial(latent_body, features=features),
        [shape((rows + rows // 2, lat), BF16), shape((rows, LANES), F32)],
        [], [], [own, got, table, latent_norm_gain[None]],
        1e6, 4,
    )
    groups = gather(block)

    chunks = rows // WINDOW
    span = rows // chunks
    group = win_query.shape[1] // win_key.shape[1]
    columns = lat_query.shape[1] // (UNROTATED_WIDTH + D_ROPE) * (rows // chunks)
    queries, key_value, inward, outward, table_a, table_b = call(
        project_body,
        [
            shape((chunks, win_key.shape[1] // DH, LANES, group * span), BF16),
            shape((rows, win_key.shape[1] + win_value.shape[1]), BF16),
            shape((WINDOW, win_key.shape[1] + win_value.shape[1]), BF16),
            shape((WINDOW, win_key.shape[1] + win_value.shape[1]), BF16),
            shape((chunks, lat + LANES, columns), BF16),
            shape((chunks, lat + LANES, columns), BF16),
        ],
        [parity[None]], [],
        [other, row_scale, table, *partial_sums, staged, key_up_weight],
        2 * rows * half * 1792, 16,
    )
    inner = lax.ppermute(inward, "sp", [(i, i ^ 1) for i in range(count) if i ^ 1 < count])

    def partner(i):
        other = i + 1 if i % 2 else i - 1
        return other if 0 <= other < count else i

    outer = lax.ppermute(
        outward, "sp", [(i, partner(i)) for i in range(count)]
    )

    sinks = jnp.broadcast_to(sink_logit[:, None] * LOG2E, (heads, LANES))
    kept = []
    assert chunks == 2
    result = None
    order = (flip, parity)
    for c, (chunk, halo) in enumerate(zip(order, (inner, outer))):
        first = groups[:1] if c == 0 else groups
        last = groups[1:] if c == 0 else []
        sizes = []
        for g in first:
            sizes += [len(g) // 2, len(g) - len(g) // 2] if len(g) > 8 else [len(g)]
        state = call(
            partial(begin_body, groups=sizes),
            [shape((16, columns), F32), shape((lat, columns), F32)],
            [chunk[None]], [], [*(b for g in first for b in g), table_a, table_b], 3e9, 32,
        )
        send, keep = call(
            partial(finish_body, groups=[len(g) for g in last], seq_total=rows * count),
            [shape((span, half), BF16), shape((span, half), F32)],
            [offset[None], part[None], chunk[None]], [],
            [
                *(b for g in last for b in g), table_a, table_b, *state, sinks, queries, halo,
                key_value, value_up_weight, out_win, out_lat,
            ],
            1e9, 16,
            [
                pltpu.VMEM((out_win.shape[0] + out_lat.shape[0], span), BF16),
                pltpu.VMEM((rows + WINDOW, key_value.shape[1]), BF16),
            ],
        )
        kept.append((chunk, keep, swap(send, "tp", 1)))
    for chunk, keep, got in kept:
        result = store(chunk, keep, got, rows, result)
    return result


def solution(mesh):
    narrow = mesh.shape["tp"] == 2
    body = per_device if narrow else per_device_wide
    return jax.shard_map(
        body,
        mesh=mesh,
        in_specs=(
            P("sp", "tp"),
            P(),
            P(None, "tp"),
            P(None, "tp"),
            P(None, "tp"),
            P("tp"),
            P(None, "tp"),
            P(),
            P(),
            P(),
            P(None, "tp"),
            P(None, "tp"),
            P("tp", None),
            P("tp", None),
        ),
        out_specs=P("sp", "tp"),
        check_vma=False,
    )
```
